512 devices in a mesh: kv: 16 (over y, x), tp: 32 (over z, core).
Axes of the slice: x: 4, y: 4, z: 16, core: 2. Of those that a mesh axis runs over, the one named last changes fastest.
Arguments:
- tokens: bfloat16 [128, 4, 4096], P(None, None, ('kv', 'tp')), may hold values from -36 to 36
- lengths: int32 [128], replicated, may hold values from 1 to 4, 224 in all
- state: float32 [128, 128, 4096], P('kv', None, 'tp'), may hold values from -0.6 to 0.6
- attn_gain: float32 [4096], P('kv'), may hold values from 0.1 to 1.9
- w_query: bfloat16 [4096, 4096], P('kv', 'tp'), may hold values from -0.09375 to 0.09375
- w_key: bfloat16 [4096, 4096], P('kv', 'tp'), may hold values from -0.09375 to 0.09375
- w_value: bfloat16 [4096, 4096], P('kv', 'tp'), may hold values from -0.09375 to 0.09375
- w_beta: bfloat16 [4096, 32], replicated, may hold values from -0.09375 to 0.09375
- w_alpha: bfloat16 [4096, 32], replicated, may hold values from -0.09375 to 0.09375
- decay_rate: float32 [32], replicated, may hold values from 0.05 to 3
- decay_bias: float32 [32], replicated, may hold values from -3 to 3
- out_gain: float32 [128], replicated, may hold values from 0.1 to 1.9
- w_out: bfloat16 [4096, 4096], P('tp', 'kv'), may hold values from -0.09375 to 0.09375
- mix_gain: float32 [4096], P('kv'), may hold values from 0.1 to 1.9
- w_gate: bfloat16 [4096, 11008], P('kv', 'tp'), may hold values from -0.09375 to 0.09375
- w_up: bfloat16 [4096, 11008], P('kv', 'tp'), may hold values from -0.09375 to 0.09375
- w_down: bfloat16 [11008, 4096], P('tp', 'kv'), may hold values from -0.0546875 to 0.0546875
Outputs:
- mixed: bfloat16 [128, 4, 4096], P(None, None, ('kv', 'tp'))
- new_state: float32 [128, 128, 4096], P('kv', None, 'tp')
The draws below stay inside these ranges and needn't reach their ends.
Inputs may be any that keep to these rules, and one draw needn't show every extreme that they name: Each sequence has 1 to 4 live tokens, the first ones of its block, and the lengths sum to 224.
All inputs are finite; a program needn't handle non-finite values.
Results may differ from the reference program's by a relative error of at most 0.015.
Values may be sent and summed in bfloat16 or wider, within the bound.
No kernel may reach another device: no remote copies, remote signals or barrier semaphores. Data moves between devices by JAX's collectives and lax.ppermute only.
A program may use at most 64 MiB of HBM per device.

```python
import math
import jax
import jax.numpy as jnp
import numpy as np
from jax import lax

D = 4096
HEADS = 32
HEAD_DIM = 128
FF = 11008
SPAN = 4
BATCH = 128
VALUE_WIDTH = 4096
N_KV = 16


def draw_tokens(key, part):
    key_base = jax.random.fold_in(key, 0)
    columns = jnp.arange(D, dtype=jnp.float32)
    block_size = D // N_KV
    within = (jnp.arange(D) % block_size).astype(jnp.float32) / block_size
    col_scale = 3.0 ** (columns / D) * 3.0 ** within
    base_draw = jnp.clip(jax.random.normal(key_base, (BATCH, SPAN, D), jnp.float32), -4.0, 4.0)
    return (base_draw * col_scale).astype(jnp.bfloat16)


def level_of(own_key, extent, pieces, low, high):
    factor_of = 1.0
    for axis_at, blocks in pieces:
        draws = jax.random.uniform(jax.random.fold_in(jax.random.fold_in(own_key, 6), axis_at), (blocks,), jnp.float32, low / len(pieces), high / len(pieces))
        factor_of = factor_of * jnp.repeat(jnp.exp(draws), extent[axis_at] // blocks).reshape((-1,) + (1,) * (len(extent) - 1 - axis_at))
    return factor_of


def split_up(amount, total, reach, lean):
    portions = [(1 << 20) // math.isqrt(grade ** lean) + 1 for grade in range(2, amount + 1)]
    spare, holding = total - reach - (amount - 1), [1] * (amount - 1)
    while spare > 0:
        movable = [i for i in range(amount - 1) if holding[i] < reach]
        mass, left = sum([portions[i] for i in movable]), spare
        for i in movable:
            addition = min(reach - holding[i], max(1, left * portions[i] // mass), spare)
            holding[i] = holding[i] + addition
            spare = spare - addition
    return np.array([reach] + holding)


def uneven(stream_key, amount, total, limit, lean):
    if amount == 2:
        one = jax.random.randint(stream_key, (), max(1, total - limit), min(limit, total - 1) + 1)
        return jnp.stack([one, total - one])
    sizes = jnp.asarray(split_up(amount, total, limit, lean), jnp.int32)
    pairs = (amount - 1) // 2
    source_of, taker = sizes[1:1 + 2 * pairs:2], sizes[2:2 + 2 * pairs:2]
    room = jnp.minimum(source_of - 1, limit - taker)
    moved = jax.random.randint(jax.random.fold_in(stream_key, 1), (pairs,), 0, 1 << 20) % (room + 1)
    sizes = sizes.at[1:1 + 2 * pairs:2].set(source_of - moved).at[2:2 + 2 * pairs:2].set(taker + moved)
    return sizes[jax.random.permutation(jax.random.fold_in(stream_key, 2), amount)]


def normal_values(own_key, extent, deviation, most, shards=(), held_as=jnp.bfloat16):
    entries = deviation * jax.random.normal(own_key, extent, jnp.float32)
    if shards:
        entries = entries * level_of(own_key, extent, shards, -0.22, 0.18)
    return jnp.clip(entries, -most, most).astype(held_as)


def setup_inputs(seed: int = 0) -> dict:
    arg_keys = jax.random.split(jax.random.key(seed), 18)
    tokens = draw_tokens(jax.random.fold_in(arg_keys[17], 71), 0)
    lengths = uneven(arg_keys[1], BATCH, BATCH * 7 // 4, SPAN, 2).astype(jnp.int32)
    state = normal_values(arg_keys[2], (BATCH, HEAD_DIM, VALUE_WIDTH), 0.1, 0.6, ((0, 16), (2, 32)), jnp.float32)
    attn_gain = jnp.clip(1.0 + 0.18 * jax.random.normal(arg_keys[3], (D,), jnp.float32), 0.1, 1.9)
    w_query = normal_values(arg_keys[4], (D, VALUE_WIDTH), D ** -0.5, 0.09375, ((0, 16), (1, 32)))
    w_key = normal_values(arg_keys[5], (D, VALUE_WIDTH), D ** -0.5, 0.09375, ((0, 16), (1, 32)))
    w_value = normal_values(arg_keys[6], (D, VALUE_WIDTH), D ** -0.5, 0.09375, ((0, 16), (1, 32)))
    w_beta = normal_values(arg_keys[7], (D, HEADS), D ** -0.5, 0.09375)
    w_alpha = normal_values(arg_keys[8], (D, HEADS), D ** -0.5, 0.09375)
    decay_rate = jnp.clip(jnp.exp(jax.random.uniform(arg_keys[9], (HEADS,), jnp.float32, math.log(0.05), math.log(3.0))), 0.05, 3.0)
    decay_bias = normal_values(arg_keys[10], (HEADS,), 1.0, 3.0, (), jnp.float32)
    out_gain = jnp.clip(1.0 + 0.18 * jax.random.normal(arg_keys[11], (HEAD_DIM,), jnp.float32), 0.1, 1.9)
    w_out = normal_values(arg_keys[12], (VALUE_WIDTH, D), VALUE_WIDTH ** -0.5, 0.09375, ((0, 32), (1, 16)))
    mix_gain = jnp.clip(1.0 + 0.18 * jax.random.normal(arg_keys[13], (D,), jnp.float32), 0.1, 1.9)
    w_gate = normal_values(arg_keys[14], (D, FF), D ** -0.5, 0.09375, ((0, 16), (1, 32)))
    w_up = normal_values(arg_keys[15], (D, FF), D ** -0.5, 0.09375, ((0, 16), (1, 32)))
    w_down = normal_values(arg_keys[16], (FF, D), FF ** -0.5, 0.0546875, ((0, 32), (1, 16)))
    return {"tokens": tokens, "lengths": lengths, "state": state, "attn_gain": attn_gain, "w_query": w_query, "w_key": w_key, "w_value": w_value, "w_beta": w_beta, "w_alpha": w_alpha, "decay_rate": decay_rate, "decay_bias": decay_bias, "out_gain": out_gain, "w_out": w_out, "mix_gain": mix_gain, "w_gate": w_gate, "w_up": w_up, "w_down": w_down}


EPSILON = 1e-06

def unit_rows(vectors):
    return vectors * lax.rsqrt(lax.optimization_barrier(jnp.sum(vectors * vectors, axis=-1, keepdims=True)) + EPSILON)

def reference(tokens, lengths, state, attn_gain, w_query, w_key, w_value, w_beta, w_alpha, decay_rate, decay_bias, out_gain, w_out, mix_gain, w_gate, w_up, w_down):
    row_total = BATCH * SPAN
    highest = lax.Precision.HIGHEST
    flat_rows = tokens.reshape(row_total, D).astype(jnp.float32)
    sq_in = lax.optimization_barrier(jnp.sum(flat_rows * flat_rows, axis=1))
    normed_in = (flat_rows * attn_gain).astype(jnp.bfloat16)
    row_scale = lax.rsqrt(sq_in / D + EPSILON)[:, None]
    query_raw = jnp.dot(normed_in, w_query, preferred_element_type=jnp.float32) * row_scale
    key_raw = jnp.dot(normed_in, w_key, preferred_element_type=jnp.float32) * row_scale
    value_rows = jnp.dot(normed_in, w_value, preferred_element_type=jnp.float32) * row_scale
    live_mask = (jnp.arange(SPAN, dtype=jnp.int32)[None, :] < lengths[:, None]).reshape(row_total, 1)
    beta = jnp.where(live_mask, jax.nn.sigmoid(jnp.dot(normed_in, w_beta, preferred_element_type=jnp.float32) * row_scale), 0.0)
    alpha_pre = jnp.dot(normed_in, w_alpha, preferred_element_type=jnp.float32) * row_scale + decay_bias
    log_decay = jnp.where(live_mask, -decay_rate * jax.nn.softplus(alpha_pre), 0.0)
    queries = unit_rows(query_raw.reshape(BATCH, SPAN, HEADS, HEAD_DIM)) * HEAD_DIM ** (-0.5)
    unit_keys = unit_rows(key_raw.reshape(BATCH, SPAN, HEADS, HEAD_DIM))
    values_split = value_rows.reshape(BATCH, SPAN, HEADS, HEAD_DIM)
    beta = beta.reshape(BATCH, SPAN, HEADS)
    log_decay = log_decay.reshape(BATCH, SPAN, HEADS)
    carried = state.reshape(BATCH, HEAD_DIM, HEADS, HEAD_DIM)
    outputs = []
    for step in range(SPAN):
        carried = carried * jnp.exp(log_decay[:, step])[:, None, :, None]
        predicted = jnp.einsum('bhd,bdhe->bhe', unit_keys[:, step], carried, precision=highest)
        update = beta[:, step][..., None] * (values_split[:, step] - predicted)
        carried = carried + jnp.einsum('bhd,bhe->bdhe', unit_keys[:, step], update, precision=highest)
        outputs.append(jnp.einsum('bhd,bdhe->bhe', queries[:, step], carried, precision=highest))
    attended = jnp.stack(outputs, axis=1)
    head_out = attended * lax.rsqrt(lax.optimization_barrier(jnp.mean(attended * attended, axis=-1, keepdims=True)) + EPSILON) * out_gain
    head_out = head_out.astype(jnp.bfloat16).reshape(row_total, VALUE_WIDTH)
    middle = (flat_rows + jnp.dot(head_out, w_out, preferred_element_type=jnp.float32)).astype(jnp.bfloat16)
    middle_f = middle.astype(jnp.float32)
    sq_mid = lax.optimization_barrier(jnp.sum(middle_f * middle_f, axis=1))
    normed_mid = (middle_f * mix_gain).astype(jnp.bfloat16)
    mid_scale = lax.rsqrt(sq_mid / D + EPSILON)[:, None]
    gate_rows = jnp.dot(normed_mid, w_gate, preferred_element_type=jnp.float32) * mid_scale
    up_rows = jnp.dot(normed_mid, w_up, preferred_element_type=jnp.float32) * mid_scale
    hidden = (jax.nn.silu(gate_rows) * up_rows).astype(jnp.bfloat16)
    result_rows = middle_f + jnp.dot(hidden, w_down, preferred_element_type=jnp.float32)
    mixed = jnp.where(live_mask, result_rows, 0.0).astype(jnp.bfloat16).reshape(BATCH, SPAN, D)
    return (mixed, carried.reshape(BATCH, HEAD_DIM, VALUE_WIDTH))
```

```python
import jax
import jax.numpy as jnp
from jax import lax
from jax.sharding import Mesh, PartitionSpec as P

D = 4096
HEAD_DIM = 128
EPSILON = 1e-06
F32 = jnp.float32
BF16 = jnp.bfloat16


def swap(tiles, axis):
    return lax.all_to_all(tiles, axis, split_axis=0, concat_axis=0, tiled=True)


def spread(shard, axis):
    return swap(jnp.broadcast_to(shard[None], (lax.axis_size(axis), *shard.shape)), axis)


def gather_features(shard):
    every = lax.all_gather(spread(shard, "z"), "c", axis=0, tiled=False)
    own, rows = shard.shape
    return jnp.swapaxes(every, 0, 1).reshape(-1, rows)


def sum_to_owner(part):
    feats, rows = part.shape
    z_count, c_count = lax.axis_size("z"), lax.axis_size("c")
    pair = lax.all_gather(part.astype(BF16), "c", axis=0, tiled=False)
    pair = pair.reshape(c_count, z_count, c_count, -1, rows)
    mine = lax.dynamic_index_in_dim(pair, lax.axis_index("c"), 2, keepdims=False)
    both = mine.astype(F32).sum(axis=0).astype(BF16)
    return swap(both, "z").astype(F32).sum(axis=0)


def unit_rows(vectors):
    return vectors * lax.rsqrt(jnp.sum(vectors * vectors, axis=-1, keepdims=True) + EPSILON)


def delta_block(queries, unit_keys, values_split, beta, log_decay, carried):
    highest = lax.Precision.HIGHEST
    seq_count, span_len, heads_here = beta.shape
    cumulative = jnp.cumsum(log_decay, axis=1)
    position = jnp.arange(span_len)
    inclusive = (position[:, None] >= position[None, :])[None, :, :, None]
    strict = (position[:, None] > position[None, :])[None, :, :, None]
    gap_matrix = cumulative[:, :, None, :] - cumulative[:, None, :, :]
    decay_matrix = jnp.where(inclusive, jnp.exp(jnp.where(inclusive, gap_matrix, 0.0)), 0.0)
    key_dots = jnp.einsum("nihd,njhd->nijh", unit_keys, unit_keys, precision=highest)
    query_dots = jnp.einsum("nihd,njhd->nijh", queries, unit_keys, precision=highest) * decay_matrix
    lower_part = jnp.where(strict, key_dots * decay_matrix * beta[:, :, None, :], 0.0)
    identity = jnp.eye(span_len, dtype=jnp.float32)
    inverse_rows = []
    for step in range(span_len):
        row_now = jnp.broadcast_to(identity[step][None, :, None], (seq_count, span_len, heads_here))
        for prior in range(step):
            row_now = row_now - lower_part[:, step, prior, :][:, None, :] * inverse_rows[prior]
        inverse_rows.append(row_now)
    inverse = jnp.stack(inverse_rows, axis=1)
    beta_value = beta[..., None] * values_split
    beta_key = (beta * jnp.exp(cumulative))[..., None] * unit_keys
    base_update = jnp.einsum("nich,nche->nihe", inverse, beta_value, precision=highest)
    key_weights = jnp.einsum("nich,nchd->nihd", inverse, beta_key, precision=highest)
    corrected = base_update - jnp.einsum("nihd,ndhe->nihe", key_weights, carried, precision=highest)
    decayed_queries = queries * jnp.exp(cumulative)[..., None]
    attended = jnp.einsum("nihd,ndhe->nihe", decayed_queries, carried, precision=highest)
    attended = attended + jnp.einsum("nijh,njhe->nihe", query_dots, corrected, precision=highest)
    block_total = cumulative[:, -1, :]
    key_tail = unit_keys * jnp.exp(block_total[:, None, :] - cumulative)[..., None]
    updated = carried * jnp.exp(block_total)[:, None, :, None]
    updated = updated + jnp.einsum("nihd,nihe->ndhe", key_tail, corrected, precision=highest)
    return (attended, updated)


def rows_dot(features_rows, weights):
    return lax.dot_general(
        features_rows, weights, (((0,), (0,)), ((), ())), preferred_element_type=F32
    )


def body(
    tokens,
    lengths,
    state,
    attn_gain,
    w_query,
    w_key,
    w_value,
    w_beta,
    w_alpha,
    decay_rate,
    decay_bias,
    out_gain,
    w_out,
    mix_gain,
    w_gate,
    w_up,
    w_down,
):
    kv_index = lax.axis_index("kv")
    kv_count = lax.axis_size("kv")
    head = lax.axis_index("z") * lax.axis_size("c") + lax.axis_index("c")
    batch_all, span_len, own_cols = tokens.shape
    row_count = batch_all * span_len
    seq_count, head_size, _ = state.shape
    local_rows = seq_count * span_len
    block_width = attn_gain.shape[0]
    slots = 256

    flat_t = tokens.reshape(row_count, own_cols).T
    gathered = gather_features(flat_t).astype(F32)
    squares_in = jnp.sum(gathered * gathered, axis=0)
    normed_in = (gathered * attn_gain[:, None]).astype(BF16)
    beta_rows = lax.dynamic_slice_in_dim(w_beta, kv_index * block_width, block_width, 0)
    alpha_rows = lax.dynamic_slice_in_dim(w_alpha, kv_index * block_width, block_width, 0)
    beta_col = lax.dynamic_slice_in_dim(beta_rows, head, 1, 1)
    alpha_col = lax.dynamic_slice_in_dim(alpha_rows, head, 1, 1)
    small = rows_dot(normed_in, jnp.concatenate([beta_col, alpha_col], axis=1)).astype(BF16)
    sent = jnp.concatenate(
        [
            rows_dot(normed_in, w_query).astype(BF16),
            rows_dot(normed_in, w_key).astype(BF16),
            rows_dot(normed_in, w_value).astype(BF16),
            small,
            squares_in.astype(BF16)[:, None],
        ],
        axis=1,
    ).reshape(kv_count, local_rows, -1)
    sums = swap(sent, "kv").astype(F32).sum(axis=0)

    row_scale = lax.rsqrt(sums[:, 386:387] / D + EPSILON)
    lengths_own = lax.dynamic_slice_in_dim(lengths, kv_index * seq_count, seq_count, 0)
    live_own = (jnp.arange(span_len, dtype=jnp.int32)[None, :] < lengths_own[:, None])[..., None]
    rate_here = lax.dynamic_slice_in_dim(decay_rate, head, 1, 0)
    bias_here = lax.dynamic_slice_in_dim(decay_bias, head, 1, 0)
    beta = jnp.where(
        live_own,
        jax.nn.sigmoid(sums[:, 384:385] * row_scale).reshape(seq_count, span_len, 1),
        0.0,
    )
    log_decay = -rate_here * jax.nn.softplus(sums[:, 385:386] * row_scale + bias_here)
    log_decay = jnp.where(live_own, log_decay.reshape(seq_count, span_len, 1), 0.0)
    split_shape = (seq_count, span_len, 1, head_size)
    queries = unit_rows((sums[:, 0:128] * row_scale).reshape(split_shape)) * HEAD_DIM ** (-0.5)
    unit_keys = unit_rows((sums[:, 128:256] * row_scale).reshape(split_shape))
    values_split = (sums[:, 256:384] * row_scale).reshape(split_shape)
    carried = state.reshape(seq_count, head_size, 1, head_size)
    attended, updated = delta_block(queries, unit_keys, values_split, beta, log_decay, carried)
    head_out = (
        attended
        * lax.rsqrt(jnp.mean(attended * attended, axis=-1, keepdims=True) + EPSILON)
        * out_gain
    )
    head_out = head_out.astype(BF16).reshape(local_rows, head_size)

    live_all = (jnp.arange(span_len, dtype=jnp.int32)[None, :] < lengths[:, None]).reshape(
        row_count
    )
    slot_index = jnp.cumsum(live_all.astype(jnp.int32)) - 1
    picker = (
        (slot_index[None, :] == jnp.arange(slots, dtype=jnp.int32)[:, None])
        & live_all[None, :]
    ).astype(BF16)
    base_rows = lax.dot_general(
        flat_t, picker, (((1,), (1,)), ((), ())), preferred_element_type=F32
    )
    heads_every = spread(head_out, "kv").reshape(row_count, head_size)
    packed_heads = jnp.dot(picker, heads_every, preferred_element_type=F32).astype(BF16)
    attn_part = lax.dot_general(
        w_out, packed_heads, (((0,), (1,)), ((), ())), preferred_element_type=F32
    )
    middle = (base_rows + sum_to_owner(attn_part)).astype(BF16)
    middle_rows = gather_features(middle).astype(F32)
    squares_mid = jnp.sum(middle_rows * middle_rows, axis=0)
    normed_mid = (middle_rows * mix_gain[:, None]).astype(BF16)
    share = jnp.concatenate(
        [
            rows_dot(normed_mid, w_gate).astype(BF16),
            rows_dot(normed_mid, w_up).astype(BF16),
            squares_mid.astype(BF16)[:, None],
        ],
        axis=1,
    ).reshape(kv_count, slots // kv_count, -1)
    share = swap(share, "kv").astype(F32).sum(axis=0)
    units = w_gate.shape[1]
    share_scale = lax.rsqrt(share[:, 2 * units :] / D + EPSILON)
    hidden = (
        jax.nn.silu(share[:, :units] * share_scale)
        * (share[:, units : 2 * units] * share_scale)
    ).astype(BF16)
    hidden_every = spread(hidden, "kv").reshape(slots, units)
    down_part = lax.dot_general(
        w_down, hidden_every, (((0,), (1,)), ((), ())), preferred_element_type=F32
    )
    result = (middle.astype(F32) + sum_to_owner(down_part)).astype(BF16)
    mixed = jnp.dot(result, picker, preferred_element_type=F32).astype(BF16)
    mixed = mixed.T.reshape(batch_all, span_len, own_cols)
    return (mixed, updated.reshape(seq_count, head_size, head_size))


def solution(mesh):
    split = Mesh(mesh.devices.reshape(mesh.shape["kv"], -1, 2), ("kv", "z", "c"))
    tp = ("z", "c")
    return jax.shard_map(
        body,
        mesh=split,
        in_specs=(
            P(None, None, ("kv", "z", "c")),
            P(),
            P("kv", None, tp),
            P("kv"),
            P("kv", tp),
            P("kv", tp),
            P("kv", tp),
            P(),
            P(),
            P(),
            P(),
            P(),
            P(tp, "kv"),
            P("kv"),
            P("kv", tp),
            P("kv", tp),
            P(tp, "kv"),
        ),
        out_specs=(P(None, None, ("kv", "z", "c")), P("kv", None, tp)),
        check_vma=False,
    )
```

```python
import jax
import jax.numpy as jnp
from jax import lax
from jax.experimental import pallas as pl
from jax.experimental.pallas import tpu as pltpu
from jax.sharding import Mesh, PartitionSpec as P

D = 4096
HEAD_DIM = 128
EPSILON = 1e-06
F32 = jnp.float32
BF16 = jnp.bfloat16


def swap(tiles, axis):
    return lax.all_to_all(tiles, axis, split_axis=0, concat_axis=0, tiled=True)


def spread(shard, axis):
    return swap(jnp.broadcast_to(shard[None], (lax.axis_size(axis), *shard.shape)), axis)


def gather_features(shard):
    return lax.all_gather(spread(shard, "z"), "c", axis=0, tiled=False)


def sum_to_owner(part):
    feats, rows = part.shape
    z_count, c_count = lax.axis_size("z"), lax.axis_size("c")
    pair = lax.all_gather(part, "c", axis=0, tiled=False)
    pair = pair.reshape(c_count, z_count, c_count, -1, rows)
    mine = lax.dynamic_index_in_dim(pair, lax.axis_index("c"), 2, keepdims=False)
    both = mine.astype(F32).sum(axis=0).astype(BF16)
    return swap(both, "z").astype(F32).sum(axis=0)


def dot(a, b, dims):
    return lax.dot_general(a, b, ((dims[:1], dims[1:]), ((), ())), preferred_element_type=F32)


def split_high_low(x):
    high = x.astype(BF16)
    return high, (x - high.astype(F32)).astype(BF16)


def full(shape_of):
    return [pl.BlockSpec(memory_space=pltpu.VMEM)] * shape_of


def features_of(ref):
    c_count, z_count = ref.shape[:2]
    return jnp.concatenate(
        [ref[c, z].astype(F32) for z in range(z_count) for c in range(c_count)], axis=0
    )


def project_kernel(
    x_ref, gain_ref, wq_ref, wk_ref, wv_ref, wb_ref, wa_ref, out_ref, wb_rows, wa_rows, sems
):
    width = gain_ref.shape[0]
    first = lax.axis_index("kv") * width
    head = lax.axis_index("z") * lax.axis_size("c") + lax.axis_index("c")
    copies = [
        pltpu.make_async_copy(src.at[pl.ds(first, width)], dst, sems.at[k])
        for k, (src, dst) in enumerate(((wb_ref, wb_rows), (wa_ref, wa_rows)))
    ]
    for copy in copies:
        copy.start()
    kv_count, local_rows, _ = out_ref.shape
    x = features_of(x_ref)
    squared = (x * x).astype(BF16)
    normed = (x * gain_ref[...]).astype(BF16)

    def put(block, value):
        out_ref[:, :, block * 128 : (block + 1) * 128] = value.astype(BF16).reshape(
            kv_count, local_rows, 128
        )

    for block, w_ref in enumerate((wq_ref, wk_ref, wv_ref)):
        put(block, dot(normed, w_ref[...], (0, 0)))
    for copy in copies:
        copy.wait()
    heads = wb_rows.shape[1]
    row = lax.broadcasted_iota(jnp.int32, (heads, 128), 0)
    lane = lax.broadcasted_iota(jnp.int32, (heads, 128), 1)
    own = row == head
    small = dot(wb_rows[...], (own & (lane == 0)).astype(BF16), (1, 0))
    small = small + dot(wa_rows[...], (own & (lane == 1)).astype(BF16), (1, 0))
    ones = (lax.broadcasted_iota(jnp.int32, (width, 128), 1) == 2).astype(BF16)
    put(3, dot(normed, small.astype(BF16), (0, 0)) + dot(squared, ones, (0, 0)))


def project(x, gain, wq, wk, wv, wb, wa, kv_count):
    rows = x.shape[-1]
    width, heads = gain.shape[0], wb.shape[1]
    return pl.pallas_call(
        project_kernel,
        out_shape=jax.ShapeDtypeStruct((kv_count, rows // kv_count, 512), BF16),
        in_specs=full(5) + [pl.BlockSpec(memory_space=pl.ANY)] * 2,
        out_specs=pl.BlockSpec(memory_space=pltpu.VMEM),
        scratch_shapes=[
            pltpu.VMEM((width, heads), BF16),
            pltpu.VMEM((width, heads), BF16),
            pltpu.SemaphoreType.DMA((2,)),
        ],
        name="project",
    )(x, gain, wq, wk, wv, wb, wa)


def delta_kernel(
    recv_ref, state_ref, lengths_ref, rate_ref, bias_ref, gain_ref, head_ref, new_ref
):
    seq_count, size, _ = state_ref.shape
    rows = recv_ref.shape[1]
    span = rows // seq_count
    first = lax.axis_index("kv") * seq_count
    head = lax.axis_index("z") * lax.axis_size("c") + lax.axis_index("c")
    sums = recv_ref[0].astype(F32)
    for k in range(1, recv_ref.shape[0]):
        sums = sums + recv_ref[k].astype(F32)

    def lanes(column):
        return jnp.broadcast_to(column, (rows, size))

    row_scale = lanes(lax.rsqrt(sums[:, 386:387] / D + EPSILON))
    row = lax.broadcasted_iota(jnp.int32, (rows, size), 0)
    step = row % span
    seq = row // span
    limit = jnp.zeros((rows, size), jnp.int32)
    for n in range(seq_count):
        limit = jnp.where(seq == n, lengths_ref[first + n], limit)
    live = step < limit
    beta = jnp.where(live, jax.nn.sigmoid(lanes(sums[:, 384:385]) * row_scale), 0.0)
    pre = lanes(sums[:, 385:386]) * row_scale + bias_ref[head]
    soft = jnp.maximum(pre, 0.0) + jnp.log1p(jnp.exp(-jnp.abs(pre)))
    log_decay = jnp.where(live, -rate_ref[head] * soft, 0.0)

    def unit(block):
        v = sums[:, block * size : (block + 1) * size] * row_scale
        return v * lax.rsqrt(jnp.sum(v * v, axis=1, keepdims=True) + EPSILON)

    queries = unit(0) * HEAD_DIM ** (-0.5)
    keys = unit(1)
    values = sums[:, 2 * size : 3 * size] * row_scale

    def back(x, d):
        return pltpu.roll(x, d, 0)

    cumulative, tail = log_decay, jnp.zeros_like(log_decay)
    gaps = [jnp.zeros_like(log_decay)]
    for d in range(1, span):
        gaps.append(jnp.where(step >= d, log_decay + back(gaps[-1], 1), 0.0))
        cumulative = cumulative + jnp.where(step >= d, back(log_decay, d), 0.0)
        tail = tail + jnp.where(step < span - d, back(log_decay, rows - d), 0.0)
    decays = [jnp.exp(g) for g in gaps]
    grown = jnp.exp(cumulative)

    both = jnp.concatenate([keys, queries], axis=0)
    both_high, both_low = split_high_low(both)
    from_state = []
    for n in range(seq_count):
        s_high, s_low = split_high_low(state_ref[n])
        from_state.append(
            dot(both_high, s_high, (1, 0))
            + dot(both_low, s_high, (1, 0))
            + dot(both_high, s_low, (1, 0))
        )
    key_state = jnp.zeros_like(keys)
    query_state = jnp.zeros_like(keys)
    for n in range(seq_count):
        key_state = jnp.where(seq == n, from_state[n][:rows], key_state)
        query_state = jnp.where(seq == n, from_state[n][rows:], query_state)

    base = beta * (values - grown * key_state)
    lower, upper = [None], []
    for d in range(span):
        shifted = back(keys, d) if d else keys
        weight = jnp.where(step >= d, decays[d], 0.0)
        upper.append(weight * jnp.sum(queries * shifted, axis=1, keepdims=True))
        if d:
            lower.append(weight * beta * jnp.sum(keys * shifted, axis=1, keepdims=True))
    update = base
    for t in range(1, span):
        now = base
        for d in range(1, t + 1):
            now = now - lower[d] * back(update, d)
        update = jnp.where(step == t, now, update)
    attended = grown * query_state + upper[0] * update
    for d in range(1, span):
        attended = attended + upper[d] * back(update, d)
    out = attended * lax.rsqrt(jnp.mean(attended * attended, axis=1, keepdims=True) + EPSILON)
    out = (out * gain_ref[...]).astype(BF16)
    for k in range(head_ref.shape[0]):
        head_ref[k] = out

    k_high, k_low = split_high_low((keys * jnp.exp(tail)).T)
    k_all = jnp.concatenate([k_high, k_low, k_high], axis=1)
    for n in range(seq_count):
        u_high, u_low = split_high_low(jnp.where(seq == n, update, 0.0))
        u_all = jnp.concatenate([u_high, u_high, u_low], axis=0)
        last = n * span + span - 1
        new_ref[n] = state_ref[n] * grown[last : last + 1, :] + dot(k_all, u_all, (1, 0))


def delta_step(recv, state, lengths, rate, bias, gain):
    kv_count, rows, _ = recv.shape
    size = state.shape[1]
    smem = pl.BlockSpec(memory_space=pltpu.SMEM)
    return pl.pallas_call(
        delta_kernel,
        out_shape=(
            jax.ShapeDtypeStruct((kv_count, rows, size), BF16),
            jax.ShapeDtypeStruct(state.shape, F32),
        ),
        in_specs=full(2) + [smem] * 3 + full(1),
        out_specs=tuple(full(2)),
        name="delta",
    )(recv, state, lengths, rate, bias, gain)


def attend_kernel(heads_ref, lengths_ref, w_ref, flat_ref, part_ref, picker_ref, base_ref):
    rows, slots = picker_ref.shape
    batch = lengths_ref.shape[1]
    span = rows // batch
    lengths = jnp.broadcast_to(lengths_ref[...].astype(F32), (batch, batch)).astype(BF16)
    before = lax.broadcasted_iota(jnp.int32, (rows, batch), 1)
    row_seq = lax.broadcasted_iota(jnp.int32, (rows, batch), 0) // span
    ahead = dot((before < row_seq).astype(BF16), lengths, (1, 1))
    limit = dot((before == row_seq).astype(BF16), lengths, (1, 1))
    step = (lax.broadcasted_iota(jnp.int32, (rows, batch), 0) % span).astype(F32)
    target = jnp.where(step < limit, ahead + step, -1.0)
    target = jnp.concatenate([target] * (slots // batch), axis=1)
    slot = lax.broadcasted_iota(jnp.int32, (rows, slots), 1).astype(F32)
    picker = (target == slot).astype(BF16)
    picker_ref[...] = picker
    heads = heads_ref[...].reshape(rows, heads_ref.shape[2])
    packed = dot(picker, heads, (0, 0)).astype(BF16)
    part_ref[...] = dot(w_ref[...], packed, (0, 1)).astype(BF16)
    base_ref[...] = dot(flat_ref[...], picker, (1, 0)).astype(BF16)


def attend(heads, lengths, w_out, flat_t, slots):
    rows = flat_t.shape[1]
    return pl.pallas_call(
        attend_kernel,
        out_shape=(
            jax.ShapeDtypeStruct((w_out.shape[1], slots), BF16),
            jax.ShapeDtypeStruct((rows, slots), BF16),
            jax.ShapeDtypeStruct((flat_t.shape[0], slots), BF16),
        ),
        in_specs=full(4),
        out_specs=tuple(full(3)),
        name="attend",
    )(heads, lengths, w_out, flat_t)


def gate_kernel(x_ref, gain_ref, wg_ref, wu_ref, out_ref):
    kv_count, local, wide = out_ref.shape
    units = wg_ref.shape[1]
    x = features_of(x_ref)
    squared = (x * x).astype(BF16)
    normed = (x * gain_ref[...]).astype(BF16)
    ones = jnp.ones((x.shape[0], 128), BF16)

    def put(at, value):
        width = value.shape[1]
        out_ref[:, :, at : at + width] = value.astype(BF16).reshape(kv_count, local, width)

    half = wide // 2
    put(0, dot(normed, wg_ref[...], (0, 0)))
    put(half, dot(normed, wu_ref[...], (0, 0)))
    put(units, dot(squared, ones, (0, 0))[:, : half - units])


def gate(x, gain, w_gate, w_up, kv_count):
    rows = x.shape[-1]
    return pl.pallas_call(
        gate_kernel,
        out_shape=jax.ShapeDtypeStruct((kv_count, rows // kv_count, 768), BF16),
        in_specs=full(4),
        out_specs=pl.BlockSpec(memory_space=pltpu.VMEM),
        name="gate",
    )(x, gain, w_gate, w_up)


def body(
    tokens,
    lengths,
    state,
    attn_gain,
    w_query,
    w_key,
    w_value,
    w_beta,
    w_alpha,
    decay_rate,
    decay_bias,
    out_gain,
    w_out,
    mix_gain,
    w_gate,
    w_up,
    w_down,
):
    kv_count = lax.axis_size("kv")
    batch_all, span_len, own_cols = tokens.shape
    row_count = batch_all * span_len
    slots = 256

    flat_t = tokens.reshape(row_count, own_cols).T
    gathered = gather_features(flat_t)
    sent = project(
        gathered, attn_gain[:, None], w_query, w_key, w_value, w_beta, w_alpha, kv_count
    )
    heads, updated = delta_step(
        swap(sent, "kv"), state, lengths, decay_rate, decay_bias, out_gain[None, :]
    )
    attn_part, picker, base_rows = attend(
        swap(heads, "kv"), lengths[None, :], w_out, flat_t, slots
    )
    middle = (base_rows.astype(F32) + sum_to_owner(attn_part)).astype(BF16)
    share = gate(gather_features(middle), mix_gain[:, None], w_gate, w_up, kv_count)
    share = swap(share, "kv").astype(F32).sum(axis=0)
    units = w_gate.shape[1]
    share_scale = lax.rsqrt(share[:, units : units + 1] / D + EPSILON)
    hidden = (
        jax.nn.silu(share[:, :units] * share_scale)
        * (share[:, 384 : 384 + units] * share_scale)
    ).astype(BF16)
    hidden_every = spread(hidden, "kv").reshape(slots, units)
    down_part = dot(w_down, hidden_every, (0, 1)).astype(BF16)
    result = (middle.astype(F32) + sum_to_owner(down_part)).astype(BF16)
    mixed = dot(result, picker, (1, 1)).astype(BF16)
    return (mixed.T.reshape(batch_all, span_len, own_cols), updated)


def solution(mesh):
    split = Mesh(mesh.devices.reshape(mesh.shape["kv"], -1, 2), ("kv", "z", "c"))
    tp = ("z", "c")
    return jax.shard_map(
        body,
        mesh=split,
        in_specs=(
            P(None, None, ("kv", "z", "c")),
            P(),
            P("kv", None, tp),
            P("kv"),
            P("kv", tp),
            P("kv", tp),
            P("kv", tp),
            P(),
            P(),
            P(),
            P(),
            P(),
            P(tp, "kv"),
            P("kv"),
            P("kv", tp),
            P("kv", tp),
            P(tp, "kv"),
        ),
        out_specs=(P(None, None, ("kv", "z", "c")), P("kv", None, tp)),
        check_vma=False,
    )
```

```python
import jax
import jax.numpy as jnp
from jax import lax
from jax.experimental import pallas as pl
from jax.experimental.pallas import tpu as pltpu
from jax.sharding import Mesh, PartitionSpec as P

D = 4096
HEAD_DIM = 128
EPSILON = 1e-06
F32 = jnp.float32
BF16 = jnp.bfloat16
PARAMS = pltpu.CompilerParams(vmem_limit_bytes=12 * 1024 * 1024)


def swap(tiles, axis):
    return lax.all_to_all(tiles, axis, split_axis=0, concat_axis=0, tiled=True)


def spread(shard, axis):
    return swap(jnp.broadcast_to(shard[None], (lax.axis_size(axis), *shard.shape)), axis)


def gather_features(shard):
    return lax.all_gather(spread(shard, "z"), "c", axis=0, tiled=False)


def pair_sum(part, core):
    feats, rows = part.shape
    z_count, c_count = lax.axis_size("z"), lax.axis_size("c")
    pair = lax.all_gather(part, "c", axis=0, tiled=False)
    pair = pair.reshape(c_count, z_count, c_count, -1, rows)
    mine = lax.dynamic_index_in_dim(pair, core, 2, keepdims=False)
    return mine.astype(F32).sum(axis=0).astype(BF16)


def dot(a, b, dims):
    return lax.dot_general(a, b, ((dims[:1], dims[1:]), ((), ())), preferred_element_type=F32)


def split_high_low(x):
    high = x.astype(BF16)
    return high, (x - high.astype(F32)).astype(BF16)


def full(shape_of):
    return [pl.BlockSpec(memory_space=pltpu.VMEM)] * shape_of


def features_of(ref, *at):
    c_count, z_count = ref.shape[:2]
    tiles = [ref[(c, z, *at)].astype(F32) for z in range(z_count) for c in range(c_count)]
    return jnp.concatenate(tiles, axis=0).T


def normed_rows(x, gain_ref):
    return (x * gain_ref[...]).astype(BF16), jnp.sum(x * x, axis=1, keepdims=True)


def project_kernel(x_ref, gain_ref, wq_ref, wk_ref, wv_ref, wb_ref, wa_ref, out_ref):
    width = gain_ref.shape[1]
    first = pl.multiple_of(lax.axis_index("kv") * width, width)
    head = lax.axis_index("z") * lax.axis_size("c") + lax.axis_index("c")
    kv_count, local_rows, _ = out_ref.shape
    span = x_ref.shape[2]
    seqs = local_rows // span
    heads = wb_ref.shape[0]
    own = lax.broadcasted_iota(jnp.int32, (heads, width), 0) == head

    def own_row(ref):
        tile = ref[:, pl.ds(first, width)].astype(F32)
        return jnp.sum(jnp.where(own, tile, 0.0), axis=0, keepdims=True)

    row = lax.broadcasted_iota(jnp.int32, (128, width), 0)
    small = jnp.where(row == 0, own_row(wb_ref), jnp.where(row == 1, own_row(wa_ref), 0.0))
    small = small.astype(BF16)
    weights = jnp.concatenate([wq_ref[...], wk_ref[...], wv_ref[...]], axis=1)
    lane = lax.broadcasted_iota(jnp.int32, (x_ref.shape[4], 128), 1)
    for t in range(span):
        normed, squares = normed_rows(features_of(x_ref, t), gain_ref)
        at = slice(t * seqs, (t + 1) * seqs)
        wide = dot(normed, weights, (1, 0))
        extra = jnp.where(lane == 2, squares, dot(normed, small, (1, 1)))
        out_ref[:, at, :384] = wide.reshape(kv_count, seqs, 384).astype(BF16)
        out_ref[:, at, 384:] = extra.reshape(kv_count, seqs, 128).astype(BF16)


def project(x, gain, wq, wk, wv, wb, wa, kv_count):
    rows = x.shape[2] * x.shape[4]
    return pl.pallas_call(
        project_kernel,
        out_shape=jax.ShapeDtypeStruct((kv_count, rows // kv_count, 512), BF16),
        in_specs=full(7),
        out_specs=pl.BlockSpec(memory_space=pltpu.VMEM),
        compiler_params=PARAMS,
        name="project",
    )(x, gain, wq, wk, wv, wb, wa)


def delta_kernel(
    recv_ref, state_ref, lengths_ref, rate_ref, bias_ref, gain_ref, head_ref, new_ref
):
    seq_count, size, _ = state_ref.shape
    rows = recv_ref.shape[1]
    span = rows // seq_count
    first = lax.axis_index("kv") * seq_count
    head = lax.axis_index("z") * lax.axis_size("c") + lax.axis_index("c")
    sums = recv_ref[0].astype(F32)
    for k in range(1, recv_ref.shape[0]):
        sums = sums + recv_ref[k].astype(F32)

    def lanes(column):
        return jnp.broadcast_to(column, (rows, size))

    row_scale = lanes(lax.rsqrt(sums[:, 386:387] / D + EPSILON))
    row = lax.broadcasted_iota(jnp.int32, (rows, size), 0)
    step = row // seq_count
    seq = row % seq_count
    limit = jnp.zeros((rows, size), jnp.int32)
    for n in range(seq_count):
        limit = jnp.where(seq == n, lengths_ref[first + n], limit)
    live = step < limit
    beta = jnp.where(live, jax.nn.sigmoid(lanes(sums[:, 384:385]) * row_scale), 0.0)
    pre = lanes(sums[:, 385:386]) * row_scale + bias_ref[head]
    soft = jnp.maximum(pre, 0.0) + jnp.log1p(jnp.exp(-jnp.abs(pre)))
    log_decay = jnp.where(live, -rate_ref[head] * soft, 0.0)

    def unit(block):
        v = sums[:, block * size : (block + 1) * size] * row_scale
        return v * lax.rsqrt(jnp.sum(v * v, axis=1, keepdims=True) + EPSILON)

    queries = unit(0) * HEAD_DIM ** (-0.5)
    keys = unit(1)
    values = sums[:, 2 * size : 3 * size] * row_scale

    def back(x, d):
        return pltpu.roll(x, d * seq_count, 0)

    cumulative, tail = log_decay, jnp.zeros_like(log_decay)
    gaps = [jnp.zeros_like(log_decay)]
    for d in range(1, span):
        gaps.append(jnp.where(step >= d, log_decay + back(gaps[-1], 1), 0.0))
        cumulative = cumulative + jnp.where(step >= d, back(log_decay, d), 0.0)
        tail = tail + jnp.where(step < span - d, back(log_decay, span - d), 0.0)
    decays = [jnp.exp(g) for g in gaps]
    grown = jnp.exp(cumulative)

    both = jnp.concatenate([keys, queries], axis=0)
    both_high, both_low = split_high_low(both)
    from_state = []
    for n in range(seq_count):
        s_high, s_low = split_high_low(state_ref[n])
        from_state.append(
            dot(both_high, s_high, (1, 0))
            + dot(both_low, s_high, (1, 0))
            + dot(both_high, s_low, (1, 0))
        )
    key_state = jnp.zeros_like(keys)
    query_state = jnp.zeros_like(keys)
    for n in range(seq_count):
        key_state = jnp.where(seq == n, from_state[n][:rows], key_state)
        query_state = jnp.where(seq == n, from_state[n][rows:], query_state)

    base = beta * (values - grown * key_state)
    lower, upper = [None], []
    for d in range(span):
        shifted = back(keys, d) if d else keys
        weight = jnp.where(step >= d, decays[d], 0.0)
        upper.append(weight * jnp.sum(queries * shifted, axis=1, keepdims=True))
        if d:
            lower.append(weight * beta * jnp.sum(keys * shifted, axis=1, keepdims=True))
    update = base
    for t in range(1, span):
        now = base
        for d in range(1, t + 1):
            now = now - lower[d] * back(update, d)
        update = jnp.where(step == t, now, update)
    attended = grown * query_state + upper[0] * update
    for d in range(1, span):
        attended = attended + upper[d] * back(update, d)
    out = attended * lax.rsqrt(jnp.mean(attended * attended, axis=1, keepdims=True) + EPSILON)
    out = (out * gain_ref[...]).astype(BF16)
    for k in range(head_ref.shape[0]):
        head_ref[k] = out

    k_high, k_low = split_high_low((keys * jnp.exp(tail)).T)
    k_all = jnp.concatenate([k_high, k_low, k_high], axis=1)
    for n in range(seq_count):
        u_high, u_low = split_high_low(jnp.where(seq == n, update, 0.0))
        u_all = jnp.concatenate([u_high, u_high, u_low], axis=0)
        last = rows - seq_count + n
        new_ref[n] = state_ref[n] * grown[last : last + 1, :] + dot(k_all, u_all, (1, 0))


def delta_step(recv, state, lengths, rate, bias, gain):
    kv_count, rows, _ = recv.shape
    size = state.shape[1]
    smem = pl.BlockSpec(memory_space=pltpu.SMEM)
    return pl.pallas_call(
        delta_kernel,
        out_shape=(
            jax.ShapeDtypeStruct((kv_count, rows, size), BF16),
            jax.ShapeDtypeStruct(state.shape, F32),
        ),
        in_specs=full(2) + [smem] * 3 + full(1),
        out_specs=tuple(full(2)),
        compiler_params=PARAMS,
        name="delta",
    )(recv, state, lengths, rate, bias, gain)


def attend_kernel(heads_ref, lengths_ref, w_ref, flat_ref, part_ref, picker_ref, base_ref):
    slots, rows = picker_ref.shape
    span, _, batch = flat_ref.shape
    kv_count, local_rows, size = heads_ref.shape
    seqs = local_rows // span
    lengths = jnp.broadcast_to(lengths_ref[...].astype(F32), (8, batch))
    above = lax.broadcasted_iota(jnp.int32, (batch, batch), 0)
    across = lax.broadcasted_iota(jnp.int32, (batch, batch), 1)
    ahead = dot(lengths.astype(BF16), (above < across).astype(BF16), (1, 0))[:1]
    slot = lax.broadcasted_iota(jnp.int32, (slots, batch), 0).astype(F32)
    for t in range(span):
        target = jnp.where(lengths[:1] > t, ahead + t, -1.0)
        picker_ref[:, t * batch : (t + 1) * batch] = (slot == target).astype(BF16)
    picker = picker_ref[...]
    heads = heads_ref[...].astype(F32)
    heads = jnp.concatenate(
        [
            heads[:, t * seqs : (t + 1) * seqs].reshape(kv_count * seqs, size)
            for t in range(span)
        ],
        axis=0,
    ).astype(BF16)
    packed = dot(picker, heads, (1, 0)).astype(BF16)
    part_ref[...] = dot(packed, w_ref[...], (1, 0)).T.astype(BF16)
    flat = jnp.concatenate([flat_ref[t] for t in range(span)], axis=1)
    base_ref[...] = dot(flat, picker, (1, 1)).astype(BF16)


def attend(heads, lengths, w_out, flat, slots):
    span, own, batch = flat.shape
    return pl.pallas_call(
        attend_kernel,
        out_shape=(
            jax.ShapeDtypeStruct((w_out.shape[1], slots), BF16),
            jax.ShapeDtypeStruct((slots, span * batch), BF16),
            jax.ShapeDtypeStruct((own, slots), BF16),
        ),
        in_specs=full(4),
        out_specs=tuple(full(3)),
        compiler_params=PARAMS,
        name="attend",
    )(heads, lengths, w_out, flat)


def gate_kernel(x_ref, gain_ref, wg_ref, wu_ref, out_ref):
    kv_count, local, wide = out_ref.shape
    units = wg_ref.shape[0]
    normed, squares = normed_rows(features_of(x_ref), gain_ref)

    def put(at, value):
        width = value.shape[1]
        out_ref[:, :, at : at + width] = value.astype(BF16).reshape(kv_count, local, width)

    half = wide // 2
    put(0, dot(normed, wg_ref[...], (1, 1)))
    put(half, dot(normed, wu_ref[...], (1, 1)))
    put(units, jnp.broadcast_to(squares, (x_ref.shape[3], half - units)))


def gate(x, gain, w_gate, w_up, kv_count):
    rows = x.shape[-1]
    return pl.pallas_call(
        gate_kernel,
        out_shape=jax.ShapeDtypeStruct((kv_count, rows // kv_count, 768), BF16),
        in_specs=full(4),
        out_specs=pl.BlockSpec(memory_space=pltpu.VMEM),
        compiler_params=PARAMS,
        name="gate",
    )(x, gain, w_gate, w_up)


def finish_kernel(recv_ref, middle_ref, picker_ref, out_ref):
    total = middle_ref[...].astype(F32)
    for k in range(recv_ref.shape[0]):
        total = total + recv_ref[k].astype(F32)
    span, _, batch = out_ref.shape
    spread_out = dot(total.astype(BF16), picker_ref[...], (1, 0)).astype(BF16)
    for t in range(span):
        out_ref[t] = spread_out[:, t * batch : (t + 1) * batch]


def finish(recv, middle, picker, span):
    own = middle.shape[0]
    return pl.pallas_call(
        finish_kernel,
        out_shape=jax.ShapeDtypeStruct((span, own, picker.shape[1] // span), BF16),
        in_specs=full(3),
        out_specs=pl.BlockSpec(memory_space=pltpu.VMEM),
        compiler_params=PARAMS,
        name="finish",
    )(recv, middle, picker)


def body(
    tokens,
    lengths,
    state,
    attn_gain,
    w_query,
    w_key,
    w_value,
    w_beta,
    w_alpha,
    decay_rate,
    decay_bias,
    out_gain,
    w_out,
    mix_gain,
    w_gate,
    w_up,
    w_down,
):
    kv_count = lax.axis_size("kv")
    slots = 256

    core = lax.axis_index("c").astype(jnp.uint32)
    flat, core = lax.optimization_barrier((tokens.transpose(1, 2, 0), core))
    sent = project(
        gather_features(flat),
        attn_gain[None, :],
        w_query,
        w_key,
        w_value,
        w_beta.T,
        w_alpha.T,
        kv_count,
    )
    heads, updated = delta_step(
        swap(sent, "kv"), state, lengths, decay_rate, decay_bias, out_gain[None, :]
    )
    attn_part, picker, base_rows = attend(
        swap(heads, "kv"), lengths[None, :], w_out, flat, slots
    )
    attn_own = swap(pair_sum(attn_part, core), "z").astype(F32).sum(axis=0)
    middle = (base_rows.astype(F32) + attn_own).astype(BF16)
    share = gate(gather_features(middle), mix_gain[None, :], w_gate.T, w_up.T, kv_count)
    share = swap(share, "kv").astype(F32).sum(axis=0)
    units = w_gate.shape[1]
    share_scale = lax.rsqrt(share[:, units : units + 1] / D + EPSILON)
    hidden = (
        jax.nn.silu(share[:, :units] * share_scale)
        * (share[:, 384 : 384 + units] * share_scale)
    ).astype(BF16)
    hidden_every = spread(hidden, "kv").reshape(slots, units)
    down_part = dot(w_down, hidden_every, (0, 1)).astype(BF16)
    mixed = finish(swap(pair_sum(down_part, core), "z"), middle, picker, flat.shape[0])
    return (mixed.transpose(2, 0, 1), updated)


def solution(mesh):
    split = Mesh(mesh.devices.reshape(mesh.shape["kv"], -1, 2), ("kv", "z", "c"))
    tp = ("z", "c")
    return jax.shard_map(
        body,
        mesh=split,
        in_specs=(
            P(None, None, ("kv", "z", "c")),
            P(),
            P("kv", None, tp),
            P("kv"),
            P("kv", tp),
            P("kv", tp),
            P("kv", tp),
            P(),
            P(),
            P(),
            P(),
            P(),
            P(tp, "kv"),
            P("kv"),
            P("kv", tp),
            P("kv", tp),
            P(tp, "kv"),
        ),
        out_specs=(P(None, None, ("kv", "z", "c")), P("kv", None, tp)),
        check_vma=False,
    )
```

```python
import jax
import jax.numpy as jnp
from jax import lax
from jax.experimental import pallas as pl
from jax.experimental.pallas import tpu as pltpu
from jax.sharding import Mesh, PartitionSpec as P

D = 4096
HEAD_DIM = 128
EPSILON = 1e-06
F32 = jnp.float32
BF16 = jnp.bfloat16
PARAMS = pltpu.CompilerParams(vmem_limit_bytes=12 * 1024 * 1024)


def swap(tiles, axis):
    return lax.all_to_all(tiles, axis, split_axis=0, concat_axis=0, tiled=True)


def spread(shard, axis):
    return swap(jnp.broadcast_to(shard[None], (lax.axis_size(axis), *shard.shape)), axis)


def gather_features(shard):
    return lax.all_gather(spread(shard, "z"), "c", axis=0, tiled=False)


def pair_sum(part, core):
    feats, rows = part.shape
    z_count, c_count = lax.axis_size("z"), lax.axis_size("c")
    pair = lax.all_gather(part, "c", axis=0, tiled=False)
    pair = pair.reshape(c_count, z_count, c_count, -1, rows)
    mine = lax.dynamic_index_in_dim(pair, core, 2, keepdims=False)
    return mine.astype(F32).sum(axis=0).astype(BF16)


def dot(a, b, dims):
    return lax.dot_general(a, b, ((dims[:1], dims[1:]), ((), ())), preferred_element_type=F32)


def split_high_low(x):
    high = x.astype(BF16)
    return high, (x - high.astype(F32)).astype(BF16)


def full(shape_of):
    return [pl.BlockSpec(memory_space=pltpu.VMEM)] * shape_of


def features_of(ref, *at):
    c_count, z_count = ref.shape[:2]
    tiles = [ref[(c, z, *at)].astype(F32) for z in range(z_count) for c in range(c_count)]
    return jnp.concatenate(tiles, axis=0).T


def normed_rows(x, gain):
    return (x * gain).astype(BF16), jnp.sum(x * x, axis=1, keepdims=True)


def prepare_kernel(
    flat_ref,
    lengths_ref,
    rate_ref,
    bias_ref,
    gain_ref,
    sent_ref,
    gain_rows_ref,
    table_ref,
):
    seqs, batch = table_ref.shape[1:]
    heads = rate_ref.shape[1]
    first = lax.axis_index("kv") * seqs
    head = lax.axis_index("z") * lax.axis_size("c") + lax.axis_index("c")
    flat = flat_ref[...]
    for k in range(sent_ref.shape[0]):
        sent_ref[k] = flat
    gain_rows_ref[...] = jnp.broadcast_to(gain_ref[...], gain_rows_ref.shape)
    lengths = jnp.broadcast_to(lengths_ref[...].astype(F32), (seqs, batch))
    own = lax.broadcasted_iota(jnp.int32, (seqs, batch), 1)
    own = own == first + lax.broadcasted_iota(jnp.int32, (seqs, batch), 0)
    mine = lax.broadcasted_iota(jnp.int32, (seqs, heads), 1) == head

    def chosen(mask, values):
        column = jnp.sum(jnp.where(mask, values, 0.0), axis=1, keepdims=True)
        return jnp.broadcast_to(column, (seqs, batch))

    table_ref[0] = lengths
    table_ref[1] = chosen(own, lengths)
    table_ref[2] = chosen(mine, jnp.broadcast_to(rate_ref[...], (seqs, heads)))
    table_ref[3] = chosen(mine, jnp.broadcast_to(bias_ref[...], (seqs, heads)))


def prepare(seqs, *arrays):
    flat, gain = arrays[0], arrays[4]
    return pl.pallas_call(
        prepare_kernel,
        out_shape=(
            jax.ShapeDtypeStruct((lax.axis_size("z"), *flat.shape), BF16),
            jax.ShapeDtypeStruct((8, gain.shape[1]), F32),
            jax.ShapeDtypeStruct((4, seqs, flat.shape[2]), F32),
        ),
        in_specs=full(len(arrays)),
        out_specs=tuple(full(3)),
        compiler_params=PARAMS,
        name="prepare",
    )(*arrays)


def project_kernel(x_ref, gain_ref, wq_ref, wk_ref, wv_ref, wb_ref, wa_ref, out_ref):
    kv_count, local_rows, _ = out_ref.shape
    span = x_ref.shape[2]
    seqs = local_rows // span
    heads = wb_ref.shape[0]
    head = lax.axis_index("z") * lax.axis_size("c") + lax.axis_index("c")
    width = gain_ref.shape[1]
    start = pl.multiple_of(lax.axis_index("kv") * width, width)
    own_head = lax.broadcasted_iota(jnp.int32, (heads, width), 0) == head

    def own_row(ref):
        tile = ref[:, pl.ds(start, width)].astype(F32)
        return jnp.sum(jnp.where(own_head, tile, 0.0), axis=0, keepdims=True)

    row = lax.broadcasted_iota(jnp.int32, (128, width), 0)
    small = jnp.where(row == 0, own_row(wb_ref), jnp.where(row == 1, own_row(wa_ref), 0.0))
    small = small.astype(BF16)
    weights = jnp.concatenate([wq_ref[...], wk_ref[...], wv_ref[...]], axis=1)
    lane = lax.broadcasted_iota(jnp.int32, (x_ref.shape[4], 128), 1)
    for t in range(span):
        normed, squares = normed_rows(features_of(x_ref, t), gain_ref[0:1])
        at = slice(t * seqs, (t + 1) * seqs)
        wide = dot(normed, weights, (1, 0))
        extra = jnp.where(lane == 2, squares, dot(normed, small, (1, 1)))
        out_ref[:, at, :384] = wide.reshape(kv_count, seqs, 384).astype(BF16)
        out_ref[:, at, 384:] = extra.reshape(kv_count, seqs, 128).astype(BF16)


def project(x, gain, wq, wk, wv, wb, wa, kv_count):
    rows = x.shape[2] * x.shape[4]
    return pl.pallas_call(
        project_kernel,
        out_shape=jax.ShapeDtypeStruct((kv_count, rows // kv_count, 512), BF16),
        in_specs=full(7),
        out_specs=pl.BlockSpec(memory_space=pltpu.VMEM),
        compiler_params=PARAMS,
        name="project",
    )(x, gain, wq, wk, wv, wb, wa)


def delta_kernel(recv_ref, state_ref, table_ref, gain_ref, head_ref, new_ref):
    seq_count, size, _ = state_ref.shape
    rows = recv_ref.shape[1]
    span = rows // seq_count
    sums = recv_ref[0].astype(F32)
    for k in range(1, recv_ref.shape[0]):
        sums = sums + recv_ref[k].astype(F32)

    def lanes(column):
        return jnp.broadcast_to(column, (rows, size))

    row_scale = lanes(lax.rsqrt(sums[:, 386:387] / D + EPSILON))
    row = lax.broadcasted_iota(jnp.int32, (rows, size), 0)
    step = row // seq_count
    seq = row % seq_count

    def every_step(k):
        return jnp.concatenate([table_ref[k]] * span, axis=0)

    live = step.astype(F32) < every_step(1)
    beta = jnp.where(live, jax.nn.sigmoid(lanes(sums[:, 384:385]) * row_scale), 0.0)
    pre = lanes(sums[:, 385:386]) * row_scale + every_step(3)
    soft = jnp.maximum(pre, 0.0) + jnp.log1p(jnp.exp(-jnp.abs(pre)))
    log_decay = jnp.where(live, -every_step(2) * soft, 0.0)

    def unit(block):
        v = sums[:, block * size : (block + 1) * size] * row_scale
        return v * lax.rsqrt(jnp.sum(v * v, axis=1, keepdims=True) + EPSILON)

    queries = unit(0) * HEAD_DIM ** (-0.5)
    keys = unit(1)
    values = sums[:, 2 * size : 3 * size] * row_scale

    def back(x, d):
        return pltpu.roll(x, d * seq_count, 0)

    cumulative, tail = log_decay, jnp.zeros_like(log_decay)
    gaps = [jnp.zeros_like(log_decay)]
    for d in range(1, span):
        gaps.append(jnp.where(step >= d, log_decay + back(gaps[-1], 1), 0.0))
        cumulative = cumulative + jnp.where(step >= d, back(log_decay, d), 0.0)
        tail = tail + jnp.where(step < span - d, back(log_decay, span - d), 0.0)
    decays = [jnp.exp(g) for g in gaps]
    grown = jnp.exp(cumulative)

    both_high, both_low = split_high_low(jnp.concatenate([keys, queries], axis=0))
    both_rows = jnp.concatenate(
        [
            jnp.concatenate([both_high, both_high], axis=1),
            jnp.concatenate([both_low, jnp.zeros_like(both_low)], axis=1),
        ],
        axis=0,
    )
    key_state = jnp.zeros_like(keys)
    query_state = jnp.zeros_like(keys)
    for n in range(0, seq_count, 2):
        halves = split_high_low(jnp.concatenate([state_ref[n], state_ref[n + 1]], axis=1))
        terms = dot(both_rows, jnp.concatenate(halves, axis=0), (1, 0))
        terms = terms[: 2 * rows] + terms[2 * rows :]
        for k in range(2):
            at = slice(k * size, (k + 1) * size)
            key_state = jnp.where(seq == n + k, terms[:rows, at], key_state)
            query_state = jnp.where(seq == n + k, terms[rows:, at], query_state)

    base = beta * (values - grown * key_state)
    lower, upper = [None], []
    for d in range(span):
        shifted = back(keys, d) if d else keys
        weight = jnp.where(step >= d, decays[d], 0.0)
        upper.append(weight * jnp.sum(queries * shifted, axis=1, keepdims=True))
        if d:
            lower.append(weight * beta * jnp.sum(keys * shifted, axis=1, keepdims=True))
    update = base
    for t in range(1, span):
        now = base
        for d in range(1, t + 1):
            now = now - lower[d] * back(update, d)
        update = jnp.where(step == t, now, update)
    attended = grown * query_state + upper[0] * update
    for d in range(1, span):
        attended = attended + upper[d] * back(update, d)
    out = attended * lax.rsqrt(jnp.mean(attended * attended, axis=1, keepdims=True) + EPSILON)
    out = (out * gain_ref[...]).astype(BF16)
    for k in range(head_ref.shape[0]):
        head_ref[k] = out

    k_high, k_low = split_high_low((keys * jnp.exp(tail)).T)
    k_all = jnp.concatenate([k_high, k_low, k_high], axis=1)
    for n in range(0, seq_count, 2):
        pair = [jnp.where(seq == n + k, update, 0.0) for k in range(2)]
        u_high, u_low = split_high_low(jnp.concatenate(pair, axis=1))
        added = dot(k_all, jnp.concatenate([u_high, u_high, u_low], axis=0), (1, 0))
        for k in range(2):
            last = rows - seq_count + n + k
            kept = state_ref[n + k] * grown[last : last + 1, :]
            new_ref[n + k] = kept + added[:, k * size : (k + 1) * size]


def delta_step(recv, state, table, gain):
    kv_count, rows, _ = recv.shape
    size = state.shape[1]
    return pl.pallas_call(
        delta_kernel,
        out_shape=(
            jax.ShapeDtypeStruct((kv_count, rows, size), BF16),
            jax.ShapeDtypeStruct(state.shape, F32),
        ),
        in_specs=full(4),
        out_specs=tuple(full(2)),
        compiler_params=PARAMS,
        name="delta",
    )(recv, state, table, gain)


def attend_kernel(
    heads_ref, table_ref, w_ref, flat_ref, gain_ref, part_ref, picker_ref, base_ref, gain_rows_ref
):
    gain_rows_ref[...] = jnp.broadcast_to(gain_ref[...], gain_rows_ref.shape)
    slots, rows = picker_ref.shape
    span, _, batch = flat_ref.shape
    kv_count, local_rows, size = heads_ref.shape
    seqs = local_rows // span
    lengths = table_ref[0]
    above = lax.broadcasted_iota(jnp.int32, (batch, batch), 0)
    across = lax.broadcasted_iota(jnp.int32, (batch, batch), 1)
    ahead = dot(lengths.astype(BF16), (above < across).astype(BF16), (1, 0))[:1]
    slot = lax.broadcasted_iota(jnp.int32, (slots, batch), 0).astype(F32)
    for t in range(span):
        target = jnp.where(lengths[:1] > t, ahead + t, -1.0)
        picker_ref[:, t * batch : (t + 1) * batch] = (slot == target).astype(BF16)
    picker = picker_ref[...]
    heads = heads_ref[...].astype(F32)
    heads = jnp.concatenate(
        [
            heads[:, t * seqs : (t + 1) * seqs].reshape(kv_count * seqs, size)
            for t in range(span)
        ],
        axis=0,
    ).astype(BF16)
    packed = dot(picker, heads, (1, 0)).astype(BF16)
    part_ref[...] = dot(packed, w_ref[...], (1, 0)).T.astype(BF16)
    flat = jnp.concatenate([flat_ref[t] for t in range(span)], axis=1)
    base_ref[...] = dot(flat, picker, (1, 1)).astype(BF16)


def attend(heads, table, w_out, flat, gain, slots):
    span, own, batch = flat.shape
    return pl.pallas_call(
        attend_kernel,
        out_shape=(
            jax.ShapeDtypeStruct((w_out.shape[1], slots), BF16),
            jax.ShapeDtypeStruct((slots, span * batch), BF16),
            jax.ShapeDtypeStruct((own, slots), BF16),
            jax.ShapeDtypeStruct((8, gain.shape[1]), F32),
        ),
        in_specs=full(5),
        out_specs=tuple(full(4)),
        compiler_params=PARAMS,
        name="attend",
    )(heads, table, w_out, flat, gain)


def gate_kernel(x_ref, gain_ref, wg_ref, wu_ref, out_ref):
    kv_count, local, wide = out_ref.shape
    units = wg_ref.shape[0]
    normed, squares = normed_rows(features_of(x_ref), gain_ref[0:1])

    def put(at, value):
        width = value.shape[1]
        out_ref[:, :, at : at + width] = value.astype(BF16).reshape(kv_count, local, width)

    half = wide // 2
    put(0, dot(normed, wg_ref[...], (1, 1)))
    put(half, dot(normed, wu_ref[...], (1, 1)))
    put(units, jnp.broadcast_to(squares, (x_ref.shape[3], half - units)))


def gate(x, gain, w_gate, w_up, kv_count):
    rows = x.shape[-1]
    return pl.pallas_call(
        gate_kernel,
        out_shape=jax.ShapeDtypeStruct((kv_count, rows // kv_count, 768), BF16),
        in_specs=full(4),
        out_specs=pl.BlockSpec(memory_space=pltpu.VMEM),
        compiler_params=PARAMS,
        name="gate",
    )(x, gain, w_gate, w_up)


def finish_kernel(recv_ref, middle_ref, picker_ref, out_ref):
    total = middle_ref[...].astype(F32)
    for k in range(recv_ref.shape[0]):
        total = total + recv_ref[k].astype(F32)
    span, _, batch = out_ref.shape
    spread_out = dot(total.astype(BF16), picker_ref[...], (1, 0)).astype(BF16)
    for t in range(span):
        out_ref[t] = spread_out[:, t * batch : (t + 1) * batch]


def finish(recv, middle, picker, span):
    own = middle.shape[0]
    return pl.pallas_call(
        finish_kernel,
        out_shape=jax.ShapeDtypeStruct((span, own, picker.shape[1] // span), BF16),
        in_specs=full(3),
        out_specs=pl.BlockSpec(memory_space=pltpu.VMEM),
        compiler_params=PARAMS,
        name="finish",
    )(recv, middle, picker)


def body(
    tokens,
    lengths,
    state,
    attn_gain,
    w_query,
    w_key,
    w_value,
    w_beta,
    w_alpha,
    decay_rate,
    decay_bias,
    out_gain,
    w_out,
    mix_gain,
    w_gate,
    w_up,
    w_down,
):
    kv_count = lax.axis_size("kv")
    slots = 256

    core = lax.axis_index("c").astype(jnp.uint32)
    flat, core = lax.optimization_barrier((tokens.transpose(1, 2, 0), core))
    sent, gain_in, table = prepare(
        state.shape[0],
        flat,
        lengths[None, :],
        decay_rate[None, :],
        decay_bias[None, :],
        attn_gain[None, :],
    )
    every = lax.all_gather(swap(sent, "z"), "c", axis=0, tiled=False)
    sums = project(every, gain_in, w_query, w_key, w_value, w_beta.T, w_alpha.T, kv_count)
    heads, updated = delta_step(swap(sums, "kv"), state, table, out_gain[None, :])
    attn_part, picker, base_rows, gain_mid = attend(
        swap(heads, "kv"), table, w_out, flat, mix_gain[None, :], slots
    )
    attn_own = swap(pair_sum(attn_part, core), "z").astype(F32).sum(axis=0)
    middle = (base_rows.astype(F32) + attn_own).astype(BF16)
    share = gate(gather_features(middle), gain_mid, w_gate.T, w_up.T, kv_count)
    share = swap(share, "kv").astype(F32).sum(axis=0)
    units = w_gate.shape[1]
    share_scale = lax.rsqrt(share[:, units : units + 1] / D + EPSILON)
    hidden = (
        jax.nn.silu(share[:, :units] * share_scale)
        * (share[:, 384 : 384 + units] * share_scale)
    ).astype(BF16)
    hidden_every = spread(hidden, "kv").reshape(slots, units)
    down_part = dot(w_down, hidden_every, (0, 1)).astype(BF16)
    mixed = finish(swap(pair_sum(down_part, core), "z"), middle, picker, flat.shape[0])
    return (mixed.transpose(2, 0, 1), updated)


def solution(mesh):
    split = Mesh(mesh.devices.reshape(mesh.shape["kv"], -1, 2), ("kv", "z", "c"))
    tp = ("z", "c")
    return jax.shard_map(
        body,
        mesh=split,
        in_specs=(
            P(None, None, ("kv", "z", "c")),
            P(),
            P("kv", None, tp),
            P("kv"),
            P("kv", tp),
            P("kv", tp),
            P("kv", tp),
            P(),
            P(),
            P(),
            P(),
            P(),
            P(tp, "kv"),
            P("kv"),
            P("kv", tp),
            P("kv", tp),
            P(tp, "kv"),
        ),
        out_specs=(P(None, None, ("kv", "z", "c")), P("kv", None, tp)),
        check_vma=False,
    )
```

```python
import jax
import jax.numpy as jnp
from jax import lax
from jax.experimental import pallas as pl
from jax.experimental.pallas import tpu as pltpu
from jax.sharding import Mesh, PartitionSpec as P

D = 4096
HEAD_DIM = 128
EPSILON = 1e-06
F32 = jnp.float32
BF16 = jnp.bfloat16
Z = ("zh", "zl")
NEAR = ("zl", "c")
PARAMS = pltpu.CompilerParams(vmem_limit_bytes=12 * 1024 * 1024)


def swap(tiles, axis):
    return lax.all_to_all(tiles, axis, split_axis=0, concat_axis=0, tiled=True)


def spread(shard, axis):
    return swap(jnp.broadcast_to(shard[None], (lax.axis_size(axis), *shard.shape)), axis)


def pair_sum(part, core):
    feats, rows = part.shape
    z_count, c_count = lax.axis_size(Z), lax.axis_size("c")
    pair = lax.all_gather(part, "c", axis=0, tiled=False)
    pair = pair.reshape(c_count, z_count, c_count, -1, rows)
    mine = lax.dynamic_index_in_dim(pair, core, 2, keepdims=False)
    return mine.astype(F32).sum(axis=0).astype(BF16)


def dot(a, b, dims):
    return lax.dot_general(a, b, ((dims[:1], dims[1:]), ((), ())), preferred_element_type=F32)


def split_high_low(x):
    high = x.astype(BF16)
    return high, (x - high.astype(F32)).astype(BF16)


def full(shape_of):
    return [pl.BlockSpec(memory_space=pltpu.VMEM)] * shape_of


def features_of(ref, *at):
    c_count, z_count = ref.shape[:2]
    tiles = [ref[(c, z, *at)].astype(F32) for z in range(z_count) for c in range(c_count)]
    return jnp.concatenate(tiles, axis=0).T


def normed_rows(x, gain):
    return (x * gain).astype(BF16), jnp.sum(x * x, axis=1, keepdims=True)


def prepare_kernel(
    flat_ref,
    lengths_ref,
    rate_ref,
    bias_ref,
    gain_in_ref,
    gain_mid_ref,
    gain_out_ref,
    sent_ref,
    gains_ref,
    table_ref,
):
    seqs, batch = table_ref.shape[1:]
    heads = rate_ref.shape[1]
    first = lax.axis_index("kv") * seqs
    head = lax.axis_index(Z) * lax.axis_size("c") + lax.axis_index("c")
    flat = flat_ref[...]
    for k in range(sent_ref.shape[0]):
        sent_ref[k] = flat
    gains_ref[0:1] = gain_in_ref[...]
    gains_ref[1:2] = gain_mid_ref[...]
    lengths = jnp.broadcast_to(lengths_ref[...].astype(F32), (seqs, batch))
    own = lax.broadcasted_iota(jnp.int32, (seqs, batch), 1)
    own = own == first + lax.broadcasted_iota(jnp.int32, (seqs, batch), 0)
    mine = lax.broadcasted_iota(jnp.int32, (seqs, heads), 1) == head

    def chosen(mask, values):
        column = jnp.sum(jnp.where(mask, values, 0.0), axis=1, keepdims=True)
        return jnp.broadcast_to(column, (seqs, batch))

    table_ref[0] = lengths
    table_ref[1] = chosen(own, lengths)
    table_ref[2] = chosen(mine, jnp.broadcast_to(rate_ref[...], (seqs, heads)))
    table_ref[3] = chosen(mine, jnp.broadcast_to(bias_ref[...], (seqs, heads)))
    table_ref[4] = jnp.broadcast_to(gain_out_ref[...], (seqs, batch))


def prepare(seqs, *arrays):
    flat, gain = arrays[0], arrays[4]
    return pl.pallas_call(
        prepare_kernel,
        out_shape=(
            jax.ShapeDtypeStruct((lax.axis_size(Z), *flat.shape), BF16),
            jax.ShapeDtypeStruct((8, gain.shape[1]), F32),
            jax.ShapeDtypeStruct((5, seqs, flat.shape[2]), F32),
        ),
        in_specs=full(len(arrays)),
        out_specs=tuple(full(3)),
        compiler_params=PARAMS,
        name="prepare",
    )(*arrays)


def project_kernel(x_ref, gain_ref, wq_ref, wk_ref, wv_ref, wb_ref, wa_ref, out_ref):
    kv_count, local_rows, _ = out_ref.shape
    span = x_ref.shape[2]
    seqs = local_rows // span
    heads = wb_ref.shape[0]
    head = lax.axis_index(Z) * lax.axis_size("c") + lax.axis_index("c")
    width = gain_ref.shape[1]
    start = pl.multiple_of(lax.axis_index("kv") * width, width)
    own_head = lax.broadcasted_iota(jnp.int32, (heads, width), 0) == head

    def own_row(ref):
        tile = ref[:, pl.ds(start, width)].astype(F32)
        return jnp.sum(jnp.where(own_head, tile, 0.0), axis=0, keepdims=True)

    row = lax.broadcasted_iota(jnp.int32, (128, width), 0)
    small = jnp.where(row == 0, own_row(wb_ref), jnp.where(row == 1, own_row(wa_ref), 0.0))
    small = small.astype(BF16)
    weights = jnp.concatenate([wq_ref[...], wk_ref[...], wv_ref[...]], axis=1)
    lane = lax.broadcasted_iota(jnp.int32, (x_ref.shape[4], 128), 1)
    for t in range(span):
        normed, squares = normed_rows(features_of(x_ref, t), gain_ref[0:1])
        at = slice(t * seqs, (t + 1) * seqs)
        wide = dot(normed, weights, (1, 0))
        extra = jnp.where(lane == 2, squares, dot(normed, small, (1, 1)))
        out_ref[:, at, :384] = wide.reshape(kv_count, seqs, 384).astype(BF16)
        out_ref[:, at, 384:] = extra.reshape(kv_count, seqs, 128).astype(BF16)


def project(x, gain, wq, wk, wv, wb, wa, kv_count):
    rows = x.shape[2] * x.shape[4]
    return pl.pallas_call(
        project_kernel,
        out_shape=jax.ShapeDtypeStruct((kv_count, rows // kv_count, 512), BF16),
        in_specs=full(7),
        out_specs=pl.BlockSpec(memory_space=pltpu.VMEM),
        compiler_params=PARAMS,
        name="project",
    )(x, gain, wq, wk, wv, wb, wa)


def delta_kernel(recv_ref, state_ref, table_ref, head_ref, new_ref):
    seq_count, size, _ = state_ref.shape
    rows = recv_ref.shape[1]
    span = rows // seq_count
    sums = recv_ref[0].astype(F32)
    for k in range(1, recv_ref.shape[0]):
        sums = sums + recv_ref[k].astype(F32)

    def lanes(column):
        return jnp.broadcast_to(column, (rows, size))

    row_scale = lanes(lax.rsqrt(sums[:, 386:387] / D + EPSILON))
    row = lax.broadcasted_iota(jnp.int32, (rows, size), 0)
    step = row // seq_count
    seq = row % seq_count

    def every_step(k):
        return jnp.concatenate([table_ref[k]] * span, axis=0)

    live = step.astype(F32) < every_step(1)
    beta = jnp.where(live, jax.nn.sigmoid(lanes(sums[:, 384:385]) * row_scale), 0.0)
    pre = lanes(sums[:, 385:386]) * row_scale + every_step(3)
    soft = jnp.maximum(pre, 0.0) + jnp.log1p(jnp.exp(-jnp.abs(pre)))
    log_decay = jnp.where(live, -every_step(2) * soft, 0.0)

    def unit(block):
        v = sums[:, block * size : (block + 1) * size] * row_scale
        return v * lax.rsqrt(jnp.sum(v * v, axis=1, keepdims=True) + EPSILON)

    queries = unit(0) * HEAD_DIM ** (-0.5)
    keys = unit(1)
    values = sums[:, 2 * size : 3 * size] * row_scale

    def back(x, d):
        return pltpu.roll(x, d * seq_count, 0)

    cumulative, tail = log_decay, jnp.zeros_like(log_decay)
    gaps = [jnp.zeros_like(log_decay)]
    for d in range(1, span):
        gaps.append(jnp.where(step >= d, log_decay + back(gaps[-1], 1), 0.0))
        cumulative = cumulative + jnp.where(step >= d, back(log_decay, d), 0.0)
        tail = tail + jnp.where(step < span - d, back(log_decay, span - d), 0.0)
    decays = [jnp.exp(g) for g in gaps]
    grown = jnp.exp(cumulative)

    both_high, both_low = split_high_low(jnp.concatenate([keys, queries], axis=0))
    both_rows = jnp.concatenate(
        [
            jnp.concatenate([both_high, both_high], axis=1),
            jnp.concatenate([both_low, jnp.zeros_like(both_low)], axis=1),
        ],
        axis=0,
    )
    key_state = jnp.zeros_like(keys)
    query_state = jnp.zeros_like(keys)
    for n in range(0, seq_count, 2):
        halves = split_high_low(jnp.concatenate([state_ref[n], state_ref[n + 1]], axis=1))
        terms = dot(both_rows, jnp.concatenate(halves, axis=0), (1, 0))
        terms = terms[: 2 * rows] + terms[2 * rows :]
        for k in range(2):
            at = slice(k * size, (k + 1) * size)
            key_state = jnp.where(seq == n + k, terms[:rows, at], key_state)
            query_state = jnp.where(seq == n + k, terms[rows:, at], query_state)

    base = beta * (values - grown * key_state)
    lower, upper = [None], []
    for d in range(span):
        shifted = back(keys, d) if d else keys
        weight = jnp.where(step >= d, decays[d], 0.0)
        upper.append(weight * jnp.sum(queries * shifted, axis=1, keepdims=True))
        if d:
            lower.append(weight * beta * jnp.sum(keys * shifted, axis=1, keepdims=True))
    update = base
    for t in range(1, span):
        now = base
        for d in range(1, t + 1):
            now = now - lower[d] * back(update, d)
        update = jnp.where(step == t, now, update)
    attended = grown * query_state + upper[0] * update
    for d in range(1, span):
        attended = attended + upper[d] * back(update, d)
    out = attended * lax.rsqrt(jnp.mean(attended * attended, axis=1, keepdims=True) + EPSILON)
    out = (out * every_step(4)).astype(BF16)
    for k in range(head_ref.shape[0]):
        head_ref[k] = out

    k_high, k_low = split_high_low((keys * jnp.exp(tail)).T)
    k_all = jnp.concatenate([k_high, k_low, k_high], axis=1)
    for n in range(0, seq_count, 2):
        pair = [jnp.where(seq == n + k, update, 0.0) for k in range(2)]
        u_high, u_low = split_high_low(jnp.concatenate(pair, axis=1))
        added = dot(k_all, jnp.concatenate([u_high, u_high, u_low], axis=0), (1, 0))
        for k in range(2):
            last = rows - seq_count + n + k
            kept = state_ref[n + k] * grown[last : last + 1, :]
            new_ref[n + k] = kept + added[:, k * size : (k + 1) * size]


def delta_step(recv, state, table):
    kv_count, rows, _ = recv.shape
    size = state.shape[1]
    return pl.pallas_call(
        delta_kernel,
        out_shape=(
            jax.ShapeDtypeStruct((kv_count, rows, size), BF16),
            jax.ShapeDtypeStruct(state.shape, F32),
        ),
        in_specs=full(3),
        out_specs=tuple(full(2)),
        compiler_params=PARAMS,
        name="delta",
    )(recv, state, table)


def attend_kernel(heads_ref, table_ref, w_ref, every_ref, part_ref, picker_ref, base_ref):
    slots, rows = picker_ref.shape
    c_count, _, span, own, batch = every_ref.shape
    kv_count, local_rows, size = heads_ref.shape
    seqs = local_rows // span
    lengths = table_ref[0]
    above = lax.broadcasted_iota(jnp.int32, (batch, batch), 0)
    across = lax.broadcasted_iota(jnp.int32, (batch, batch), 1)
    ahead = dot(lengths.astype(BF16), (above < across).astype(BF16), (1, 0))[:1]
    slot = lax.broadcasted_iota(jnp.int32, (slots, batch), 0).astype(F32)
    for t in range(span):
        target = jnp.where(lengths[:1] > t, ahead + t, -1.0)
        picker_ref[:, t * batch : (t + 1) * batch] = (slot == target).astype(BF16)
    picker = picker_ref[...]
    heads = heads_ref[...].astype(F32)
    heads = jnp.concatenate(
        [
            heads[:, t * seqs : (t + 1) * seqs].reshape(kv_count * seqs, size)
            for t in range(span)
        ],
        axis=0,
    ).astype(BF16)
    packed = dot(picker, heads, (1, 0)).astype(BF16)
    part_ref[...] = dot(packed, w_ref[...], (1, 0)).T.astype(BF16)
    near = lax.axis_index("zl") * c_count + lax.axis_index("c")
    chips = base_ref.shape[0] // (own * c_count)
    tiles = [
        jnp.concatenate([every_ref[c, near * chips + k, t] for t in range(span)], axis=1)
        for k in range(chips)
        for c in range(c_count)
    ]
    tiles = jnp.concatenate([tile.astype(F32) for tile in tiles], axis=0).astype(BF16)
    base_ref[...] = dot(tiles, picker, (1, 1)).astype(BF16)


def attend(heads, table, w_out, every, slots, near_feats):
    _, _, span, _, batch = every.shape
    return pl.pallas_call(
        attend_kernel,
        out_shape=(
            jax.ShapeDtypeStruct((w_out.shape[1], slots), BF16),
            jax.ShapeDtypeStruct((slots, span * batch), BF16),
            jax.ShapeDtypeStruct((near_feats, slots), BF16),
        ),
        in_specs=full(4),
        out_specs=tuple(full(3)),
        compiler_params=PARAMS,
        name="attend",
    )(heads, table, w_out, every)


def gate_kernel(x_ref, gain_ref, wg_ref, wu_ref, out_ref, own_ref):
    kv_count, local, wide = out_ref.shape
    units = wg_ref.shape[0]
    near_count, feats, slots = x_ref.shape
    x = x_ref[...].astype(F32).reshape(near_count * feats, slots)
    own = own_ref.shape[0]
    first = ((lax.axis_index(Z)) * lax.axis_size("c") + lax.axis_index("c")) * own
    chunk = x_ref[first // feats].astype(F32)
    mine = chunk[:own]
    for k in range(1, feats // own):
        mine = jnp.where(first % feats == k * own, chunk[k * own : (k + 1) * own], mine)
    own_ref[...] = mine.astype(BF16)
    normed, squares = normed_rows(x.T, gain_ref[1:2])

    def put(at, value):
        width = value.shape[1]
        out_ref[:, :, at : at + width] = value.astype(BF16).reshape(kv_count, local, width)

    half = wide // 2
    put(0, dot(normed, wg_ref[...], (1, 1)))
    put(half, dot(normed, wu_ref[...], (1, 1)))
    put(units, jnp.broadcast_to(squares, (slots, half - units)))


def gate(x, gain, w_gate, w_up, kv_count, own):
    rows = x.shape[-1]
    return pl.pallas_call(
        gate_kernel,
        out_shape=(
            jax.ShapeDtypeStruct((kv_count, rows // kv_count, 768), BF16),
            jax.ShapeDtypeStruct((own, rows), BF16),
        ),
        in_specs=full(4),
        out_specs=tuple(full(2)),
        compiler_params=PARAMS,
        name="gate",
    )(x, gain, w_gate, w_up)


def finish_kernel(recv_ref, middle_ref, picker_ref, out_ref):
    total = middle_ref[...].astype(F32)
    for k in range(recv_ref.shape[0]):
        total = total + recv_ref[k].astype(F32)
    span, _, batch = out_ref.shape
    spread_out = dot(total.astype(BF16), picker_ref[...], (1, 0)).astype(BF16)
    for t in range(span):
        out_ref[t] = spread_out[:, t * batch : (t + 1) * batch]


def finish(recv, middle, picker, span):
    own = middle.shape[0]
    return pl.pallas_call(
        finish_kernel,
        out_shape=jax.ShapeDtypeStruct((span, own, picker.shape[1] // span), BF16),
        in_specs=full(3),
        out_specs=pl.BlockSpec(memory_space=pltpu.VMEM),
        compiler_params=PARAMS,
        name="finish",
    )(recv, middle, picker)


def body(
    tokens,
    lengths,
    state,
    attn_gain,
    w_query,
    w_key,
    w_value,
    w_beta,
    w_alpha,
    decay_rate,
    decay_bias,
    out_gain,
    w_out,
    mix_gain,
    w_gate,
    w_up,
    w_down,
):
    kv_count = lax.axis_size("kv")
    slots = 256

    core = lax.axis_index("c").astype(jnp.uint32)
    flat, core = lax.optimization_barrier((tokens.transpose(1, 2, 0), core))
    sent, gains, table = prepare(
        state.shape[0],
        flat,
        lengths[None, :],
        decay_rate[None, :],
        decay_bias[None, :],
        attn_gain[None, :],
        mix_gain[None, :],
        out_gain[None, :],
    )
    every = lax.all_gather(swap(sent, Z), "c", axis=0, tiled=False)
    sums = project(every, gains, w_query, w_key, w_value, w_beta.T, w_alpha.T, kv_count)
    heads, updated = delta_step(swap(sums, "kv"), state, table)
    near_count = lax.axis_size(NEAR)
    attn_part, picker, base_rows = attend(
        swap(heads, "kv"), table, w_out, every, slots, w_out.shape[1] // near_count
    )
    near_sum = swap(attn_part.reshape(near_count, -1, slots), NEAR).astype(F32).sum(axis=0)
    far_terms = spread(near_sum.astype(BF16), "zh").astype(F32).sum(axis=0)
    middle_rows = spread((base_rows.astype(F32) + far_terms).astype(BF16), NEAR)
    share, middle = gate(middle_rows, gains, w_gate.T, w_up.T, kv_count, flat.shape[1])
    share = swap(share, "kv").astype(F32).sum(axis=0)
    units = w_gate.shape[1]
    share_scale = lax.rsqrt(share[:, units : units + 1] / D + EPSILON)
    hidden = (
        jax.nn.silu(share[:, :units] * share_scale)
        * (share[:, 384 : 384 + units] * share_scale)
    ).astype(BF16)
    hidden_every = spread(hidden, "kv").reshape(slots, units)
    down_part = dot(w_down, hidden_every, (0, 1)).astype(BF16)
    mixed = finish(swap(pair_sum(down_part, core), Z), middle, picker, flat.shape[0])
    return (mixed.transpose(2, 0, 1), updated)


def solution(mesh):
    tp = ("zh", "zl", "c")
    split = Mesh(mesh.devices.reshape(mesh.shape["kv"], -1, 4, 2), ("kv", *tp))
    return jax.shard_map(
        body,
        mesh=split,
        in_specs=(
            P(None, None, ("kv", *tp)),
            P(),
            P("kv", None, tp),
            P("kv"),
            P("kv", tp),
            P("kv", tp),
            P("kv", tp),
            P(),
            P(),
            P(),
            P(),
            P(),
            P(tp, "kv"),
            P("kv"),
            P("kv", tp),
            P("kv", tp),
            P(tp, "kv"),
        ),
        out_specs=(P(None, None, ("kv", *tp)), P("kv", None, tp)),
        check_vma=False,
    )
```

```python
import jax
import jax.numpy as jnp
from jax import lax
from jax.experimental import pallas as pl
from jax.experimental.pallas import tpu as pltpu
from jax.sharding import Mesh, PartitionSpec as P

D = 4096
HEAD_DIM = 128
EPSILON = 1e-06
F32 = jnp.float32
BF16 = jnp.bfloat16
Z = "z"
COST = pl.CostEstimate(flops=1 << 28, bytes_accessed=1 << 21, transcendentals=0)
PARAMS = pltpu.CompilerParams(vmem_limit_bytes=12 * 1024 * 1024)


def swap(tiles, axis):
    return lax.all_to_all(tiles, axis, split_axis=0, concat_axis=0, tiled=True)


def spread(shard, axis):
    return swap(jnp.broadcast_to(shard[None], (lax.axis_size(axis), *shard.shape)), axis)


def pair_sum(part, core):
    feats, rows = part.shape
    z_count, c_count = lax.axis_size(Z), lax.axis_size("c")
    pair = lax.all_gather(part, "c", axis=0, tiled=False)
    pair = pair.reshape(c_count, z_count, c_count, -1, rows)
    mine = lax.dynamic_index_in_dim(pair, core, 2, keepdims=False)
    return mine.astype(F32).sum(axis=0).astype(BF16)


def dot(a, b, dims):
    return lax.dot_general(a, b, ((dims[:1], dims[1:]), ((), ())), preferred_element_type=F32)


def split_high_low(x):
    high = x.astype(BF16)
    return high, (x - high.astype(F32)).astype(BF16)


def full(shape_of):
    return [pl.BlockSpec(memory_space=pltpu.VMEM)] * shape_of


def features_of(ref, *at):
    c_count, z_count = ref.shape[:2]
    tiles = [ref[(c, z, *at)].astype(F32) for z in range(z_count) for c in range(c_count)]
    return jnp.concatenate(tiles, axis=0).T


def normed_rows(x, gain):
    return (x * gain).astype(BF16), jnp.sum(x * x, axis=1, keepdims=True)


def prepare_kernel(
    flat_ref,
    lengths_ref,
    rate_ref,
    bias_ref,
    gain_in_ref,
    gain_mid_ref,
    gain_out_ref,
    sent_ref,
    gains_ref,
    table_ref,
):
    seqs, batch = table_ref.shape[1:]
    heads = rate_ref.shape[1]
    first = lax.axis_index("kv") * seqs
    head = lax.axis_index(Z) * lax.axis_size("c") + lax.axis_index("c")
    flat = flat_ref[...]
    for k in range(sent_ref.shape[0]):
        sent_ref[k] = flat
    gains_ref[0:1] = gain_in_ref[...]
    gains_ref[1:2] = gain_mid_ref[...]
    lengths = jnp.broadcast_to(lengths_ref[...].astype(F32), (seqs, batch))
    own = lax.broadcasted_iota(jnp.int32, (seqs, batch), 1)
    own = own == first + lax.broadcasted_iota(jnp.int32, (seqs, batch), 0)
    mine = lax.broadcasted_iota(jnp.int32, (seqs, heads), 1) == head

    def chosen(mask, values):
        column = jnp.sum(jnp.where(mask, values, 0.0), axis=1, keepdims=True)
        return jnp.broadcast_to(column, (seqs, batch))

    table_ref[0] = lengths
    table_ref[1] = chosen(own, lengths)
    table_ref[2] = chosen(mine, jnp.broadcast_to(rate_ref[...], (seqs, heads)))
    table_ref[3] = chosen(mine, jnp.broadcast_to(bias_ref[...], (seqs, heads)))
    table_ref[4] = jnp.broadcast_to(gain_out_ref[...], (seqs, batch))


def prepare(seqs, *arrays):
    flat, gain = arrays[0], arrays[4]
    return pl.pallas_call(
        prepare_kernel,
        out_shape=(
            jax.ShapeDtypeStruct((lax.axis_size(Z), *flat.shape), BF16),
            jax.ShapeDtypeStruct((8, gain.shape[1]), F32),
            jax.ShapeDtypeStruct((5, seqs, flat.shape[2]), F32),
        ),
        in_specs=full(len(arrays)),
        out_specs=tuple(full(3)),
        compiler_params=PARAMS,
        cost_estimate=COST,
        name="prepare",
    )(*arrays)


def project_kernel(x_ref, gain_ref, wq_ref, wk_ref, wv_ref, wb_ref, wa_ref, out_ref):
    kv_count, local_rows, _ = out_ref.shape
    span = x_ref.shape[2]
    seqs = local_rows // span
    heads = wb_ref.shape[0]
    head = lax.axis_index(Z) * lax.axis_size("c") + lax.axis_index("c")
    width = gain_ref.shape[1]
    start = pl.multiple_of(lax.axis_index("kv") * width, width)
    own_head = lax.broadcasted_iota(jnp.int32, (heads, width), 0) == head

    def own_row(ref):
        tile = ref[:, pl.ds(start, width)].astype(F32)
        return jnp.sum(jnp.where(own_head, tile, 0.0), axis=0, keepdims=True)

    row = lax.broadcasted_iota(jnp.int32, (128, width), 0)
    small = jnp.where(row == 0, own_row(wb_ref), jnp.where(row == 1, own_row(wa_ref), 0.0))
    small = small.astype(BF16)
    weights = jnp.concatenate([wq_ref[...], wk_ref[...], wv_ref[...]], axis=1)
    lane = lax.broadcasted_iota(jnp.int32, (x_ref.shape[4], 128), 1)
    for t in range(span):
        normed, squares = normed_rows(features_of(x_ref, t), gain_ref[0:1])
        at = slice(t * seqs, (t + 1) * seqs)
        wide = dot(normed, weights, (1, 0))
        extra = jnp.where(lane == 2, squares, dot(normed, small, (1, 1)))
        out_ref[:, at, :384] = wide.reshape(kv_count, seqs, 384).astype(BF16)
        out_ref[:, at, 384:] = extra.reshape(kv_count, seqs, 128).astype(BF16)


def project(x, gain, wq, wk, wv, wb, wa, kv_count):
    rows = x.shape[2] * x.shape[4]
    return pl.pallas_call(
        project_kernel,
        out_shape=jax.ShapeDtypeStruct((kv_count, rows // kv_count, 512), BF16),
        in_specs=full(7),
        out_specs=pl.BlockSpec(memory_space=pltpu.VMEM),
        compiler_params=PARAMS,
        name="project",
    )(x, gain, wq, wk, wv, wb, wa)


def delta_kernel(recv_ref, state_ref, table_ref, head_ref, new_ref):
    seq_count, size, _ = state_ref.shape
    rows = recv_ref.shape[1]
    span = rows // seq_count
    sums = recv_ref[0].astype(F32)
    for k in range(1, recv_ref.shape[0]):
        sums = sums + recv_ref[k].astype(F32)

    def lanes(column):
        return jnp.broadcast_to(column, (rows, size))

    row_scale = lanes(lax.rsqrt(sums[:, 386:387] / D + EPSILON))
    row = lax.broadcasted_iota(jnp.int32, (rows, size), 0)
    step = row // seq_count
    seq = row % seq_count

    def every_step(k):
        return jnp.concatenate([table_ref[k]] * span, axis=0)

    live = step.astype(F32) < every_step(1)
    beta = jnp.where(live, jax.nn.sigmoid(lanes(sums[:, 384:385]) * row_scale), 0.0)
    pre = lanes(sums[:, 385:386]) * row_scale + every_step(3)
    soft = jnp.maximum(pre, 0.0) + jnp.log1p(jnp.exp(-jnp.abs(pre)))
    log_decay = jnp.where(live, -every_step(2) * soft, 0.0)

    def unit(block):
        v = sums[:, block * size : (block + 1) * size] * row_scale
        return v * lax.rsqrt(jnp.sum(v * v, axis=1, keepdims=True) + EPSILON)

    queries = unit(0) * HEAD_DIM ** (-0.5)
    keys = unit(1)
    values = sums[:, 2 * size : 3 * size] * row_scale

    def back(x, d):
        return pltpu.roll(x, d * seq_count, 0)

    cumulative, tail = log_decay, jnp.zeros_like(log_decay)
    gaps = [jnp.zeros_like(log_decay)]
    for d in range(1, span):
        gaps.append(jnp.where(step >= d, log_decay + back(gaps[-1], 1), 0.0))
        cumulative = cumulative + jnp.where(step >= d, back(log_decay, d), 0.0)
        tail = tail + jnp.where(step < span - d, back(log_decay, span - d), 0.0)
    decays = [jnp.exp(g) for g in gaps]
    grown = jnp.exp(cumulative)

    both_high, both_low = split_high_low(jnp.concatenate([keys, queries], axis=0))
    both_rows = jnp.concatenate(
        [
            jnp.concatenate([both_high, both_high], axis=1),
            jnp.concatenate([both_low, jnp.zeros_like(both_low)], axis=1),
        ],
        axis=0,
    )
    key_state = jnp.zeros_like(keys)
    query_state = jnp.zeros_like(keys)
    for n in range(0, seq_count, 2):
        halves = split_high_low(jnp.concatenate([state_ref[n], state_ref[n + 1]], axis=1))
        terms = dot(both_rows, jnp.concatenate(halves, axis=0), (1, 0))
        terms = terms[: 2 * rows] + terms[2 * rows :]
        for k in range(2):
            at = slice(k * size, (k + 1) * size)
            key_state = jnp.where(seq == n + k, terms[:rows, at], key_state)
            query_state = jnp.where(seq == n + k, terms[rows:, at], query_state)

    base = beta * (values - grown * key_state)
    lower, upper = [None], []
    for d in range(span):
        shifted = back(keys, d) if d else keys
        weight = jnp.where(step >= d, decays[d], 0.0)
        upper.append(weight * jnp.sum(queries * shifted, axis=1, keepdims=True))
        if d:
            lower.append(weight * beta * jnp.sum(keys * shifted, axis=1, keepdims=True))
    update = base
    for t in range(1, span):
        now = base
        for d in range(1, t + 1):
            now = now - lower[d] * back(update, d)
        update = jnp.where(step == t, now, update)
    attended = grown * query_state + upper[0] * update
    for d in range(1, span):
        attended = attended + upper[d] * back(update, d)
    out = attended * lax.rsqrt(jnp.mean(attended * attended, axis=1, keepdims=True) + EPSILON)
    out = (out * every_step(4)).astype(BF16)
    for k in range(head_ref.shape[0]):
        head_ref[k] = out

    k_high, k_low = split_high_low((keys * jnp.exp(tail)).T)
    k_all = jnp.concatenate([k_high, k_low, k_high], axis=1)
    for n in range(0, seq_count, 2):
        pair = [jnp.where(seq == n + k, update, 0.0) for k in range(2)]
        u_high, u_low = split_high_low(jnp.concatenate(pair, axis=1))
        added = dot(k_all, jnp.concatenate([u_high, u_high, u_low], axis=0), (1, 0))
        for k in range(2):
            last = rows - seq_count + n + k
            kept = state_ref[n + k] * grown[last : last + 1, :]
            new_ref[n + k] = kept + added[:, k * size : (k + 1) * size]


def delta_step(recv, state, table):
    kv_count, rows, _ = recv.shape
    size = state.shape[1]
    return pl.pallas_call(
        delta_kernel,
        out_shape=(
            jax.ShapeDtypeStruct((kv_count, rows, size), BF16),
            jax.ShapeDtypeStruct(state.shape, F32),
        ),
        in_specs=full(3),
        out_specs=tuple(full(2)),
        compiler_params=PARAMS,
        name="delta",
    )(recv, state, table)


def attend_kernel(heads_ref, table_ref, w_ref, flat_ref, part_ref, picker_ref, base_ref):
    slots, rows = picker_ref.shape
    span, _, batch = flat_ref.shape
    kv_count, local_rows, size = heads_ref.shape
    seqs = local_rows // span
    lengths = table_ref[0]
    above = lax.broadcasted_iota(jnp.int32, (batch, batch), 0)
    across = lax.broadcasted_iota(jnp.int32, (batch, batch), 1)
    ahead = dot(lengths.astype(BF16), (above < across).astype(BF16), (1, 0))[:1]
    slot = lax.broadcasted_iota(jnp.int32, (slots, batch), 0).astype(F32)
    for t in range(span):
        target = jnp.where(lengths[:1] > t, ahead + t, -1.0)
        picker_ref[:, t * batch : (t + 1) * batch] = (slot == target).astype(BF16)
    picker = picker_ref[...]
    heads = heads_ref[...].astype(F32)
    heads = jnp.concatenate(
        [
            heads[:, t * seqs : (t + 1) * seqs].reshape(kv_count * seqs, size)
            for t in range(span)
        ],
        axis=0,
    ).astype(BF16)
    packed = dot(picker, heads, (1, 0)).astype(BF16)
    part_ref[...] = dot(packed, w_ref[...], (1, 0)).T.astype(BF16)
    flat = jnp.concatenate([flat_ref[t] for t in range(span)], axis=1)
    base_ref[...] = dot(flat, picker, (1, 1)).astype(BF16)


def attend(heads, table, w_out, flat, slots):
    span, own, batch = flat.shape
    return pl.pallas_call(
        attend_kernel,
        out_shape=(
            jax.ShapeDtypeStruct((w_out.shape[1], slots), BF16),
            jax.ShapeDtypeStruct((slots, span * batch), BF16),
            jax.ShapeDtypeStruct((own, slots), BF16),
        ),
        in_specs=full(4),
        out_specs=tuple(full(3)),
        compiler_params=PARAMS,
        name="attend",
    )(heads, table, w_out, flat)


def gate_kernel(x_ref, gain_ref, wg_ref, wu_ref, out_ref):
    kv_count, local, wide = out_ref.shape
    units = wg_ref.shape[0]
    normed, squares = normed_rows(features_of(x_ref), gain_ref[1:2])

    def put(at, value):
        width = value.shape[1]
        out_ref[:, :, at : at + width] = value.astype(BF16).reshape(kv_count, local, width)

    half = wide // 2
    put(0, dot(normed, wg_ref[...], (1, 1)))
    put(half, dot(normed, wu_ref[...], (1, 1)))
    put(units, jnp.broadcast_to(squares, (x_ref.shape[3], half - units)))


def gate(x, gain, w_gate, w_up, kv_count):
    rows = x.shape[-1]
    return pl.pallas_call(
        gate_kernel,
        out_shape=jax.ShapeDtypeStruct((kv_count, rows // kv_count, 768), BF16),
        in_specs=full(4),
        out_specs=pl.BlockSpec(memory_space=pltpu.VMEM),
        compiler_params=PARAMS,
        name="gate",
    )(x, gain, w_gate, w_up)


def finish_kernel(recv_ref, middle_ref, picker_ref, out_ref):
    total = middle_ref[...].astype(F32)
    for k in range(recv_ref.shape[0]):
        total = total + recv_ref[k].astype(F32)
    span, _, batch = out_ref.shape
    spread_out = dot(total.astype(BF16), picker_ref[...], (1, 0)).astype(BF16)
    for t in range(span):
        out_ref[t] = spread_out[:, t * batch : (t + 1) * batch]


def finish(recv, middle, picker, span):
    own = middle.shape[0]
    return pl.pallas_call(
        finish_kernel,
        out_shape=jax.ShapeDtypeStruct((span, own, picker.shape[1] // span), BF16),
        in_specs=full(3),
        out_specs=pl.BlockSpec(memory_space=pltpu.VMEM),
        compiler_params=PARAMS,
        name="finish",
    )(recv, middle, picker)


def body(
    tokens,
    lengths,
    state,
    attn_gain,
    w_query,
    w_key,
    w_value,
    w_beta,
    w_alpha,
    decay_rate,
    decay_bias,
    out_gain,
    w_out,
    mix_gain,
    w_gate,
    w_up,
    w_down,
):
    kv_count = lax.axis_size("kv")
    slots = 256

    core = lax.axis_index("c").astype(jnp.uint32)
    flat, core = lax.optimization_barrier((tokens.transpose(1, 2, 0), core))
    sent, gains, table = prepare(
        state.shape[0],
        flat,
        lengths[None, :],
        decay_rate[None, :],
        decay_bias[None, :],
        attn_gain[None, :],
        mix_gain[None, :],
        out_gain[None, :],
    )
    every = lax.all_gather(swap(sent, Z), "c", axis=0, tiled=False)
    sums = project(every, gains, w_query, w_key, w_value, w_beta.T, w_alpha.T, kv_count)
    heads, updated = delta_step(swap(sums, "kv"), state, table)
    attn_part, picker, base_rows = attend(swap(heads, "kv"), table, w_out, flat, slots)
    attn_own = swap(pair_sum(attn_part, core), Z).astype(F32).sum(axis=0)
    middle = (base_rows.astype(F32) + attn_own).astype(BF16)
    middle_rows = lax.all_gather(spread(middle, Z), "c", axis=0, tiled=False)
    share = gate(middle_rows, gains, w_gate.T, w_up.T, kv_count)
    share = swap(share, "kv").astype(F32).sum(axis=0)
    units = w_gate.shape[1]
    share_scale = lax.rsqrt(share[:, units : units + 1] / D + EPSILON)
    hidden = (
        jax.nn.silu(share[:, :units] * share_scale)
        * (share[:, 384 : 384 + units] * share_scale)
    ).astype(BF16)
    hidden_every = spread(hidden, "kv").reshape(slots, units)
    down_part = dot(w_down, hidden_every, (0, 1)).astype(BF16)
    mixed = finish(swap(pair_sum(down_part, core), Z), middle, picker, flat.shape[0])
    return (mixed.transpose(2, 0, 1), updated)


def solution(mesh):
    tp = ("z", "c")
    split = Mesh(mesh.devices.reshape(mesh.shape["kv"], -1, 2), ("kv", *tp))
    return jax.shard_map(
        body,
        mesh=split,
        in_specs=(
            P(None, None, ("kv", *tp)),
            P(),
            P("kv", None, tp),
            P("kv"),
            P("kv", tp),
            P("kv", tp),
            P("kv", tp),
            P(),
            P(),
            P(),
            P(),
            P(),
            P(tp, "kv"),
            P("kv"),
            P("kv", tp),
            P("kv", tp),
            P(tp, "kv"),
        ),
        out_specs=(P(None, None, ("kv", *tp)), P("kv", None, tp)),
        check_vma=False,
    )
```

```python
import jax
import jax.numpy as jnp
from jax import lax
from jax.experimental import pallas as pl
from jax.experimental.pallas import tpu as pltpu
from jax.sharding import Mesh, PartitionSpec as P

D = 4096
HEAD_DIM = 128
EPSILON = 1e-06
F32 = jnp.float32
BF16 = jnp.bfloat16
Z = "z"
COST = pl.CostEstimate(flops=1 << 28, bytes_accessed=1 << 21, transcendentals=0)
PARAMS = pltpu.CompilerParams(vmem_limit_bytes=12 * 1024 * 1024)


def swap(tiles, axis):
    return lax.all_to_all(tiles, axis, split_axis=0, concat_axis=0, tiled=True)


def spread(shard, axis):
    return swap(jnp.broadcast_to(shard[None], (lax.axis_size(axis), *shard.shape)), axis)


def pair_sum(part, core):
    feats, rows = part.shape
    z_count, c_count = lax.axis_size(Z), lax.axis_size("c")
    pair = lax.all_gather(part, "c", axis=0, tiled=False)
    pair = pair.reshape(c_count, z_count, c_count, -1, rows)
    mine = lax.dynamic_index_in_dim(pair, core, 2, keepdims=False)
    return mine.astype(F32).sum(axis=0).astype(BF16)


def dot(a, b, dims):
    return lax.dot_general(a, b, ((dims[:1], dims[1:]), ((), ())), preferred_element_type=F32)


def split_high_low(x):
    high = x.astype(BF16)
    return high, (x - high.astype(F32)).astype(BF16)


def full(shape_of):
    return [pl.BlockSpec(memory_space=pltpu.VMEM)] * shape_of


def features_of(ref, *at):
    c_count, z_count = ref.shape[:2]
    tiles = [ref[(c, z, *at)].astype(F32) for z in range(z_count) for c in range(c_count)]
    return jnp.concatenate(tiles, axis=0).T


def normed_rows(x, gain):
    return (x * gain).astype(BF16), jnp.sum(x * x, axis=1, keepdims=True)


def prepare_kernel(
    flat_ref,
    lengths_ref,
    rate_ref,
    bias_ref,
    gain_in_ref,
    gain_mid_ref,
    gain_out_ref,
    sent_ref,
    gains_ref,
    table_ref,
    picker_ref,
):
    seqs, batch = table_ref.shape[1:]
    span = flat_ref.shape[0]
    slots = picker_ref.shape[0]
    heads = rate_ref.shape[1]
    first = lax.axis_index("kv") * seqs
    head = lax.axis_index(Z) * lax.axis_size("c") + lax.axis_index("c")
    gains_ref[0:1] = gain_in_ref[...]
    gains_ref[1:2] = gain_mid_ref[...]
    lengths = jnp.broadcast_to(lengths_ref[...].astype(F32), (seqs, batch))
    own = lax.broadcasted_iota(jnp.int32, (seqs, batch), 1)
    own = own == first + lax.broadcasted_iota(jnp.int32, (seqs, batch), 0)
    mine = lax.broadcasted_iota(jnp.int32, (seqs, heads), 1) == head

    def chosen(mask, values):
        column = jnp.sum(jnp.where(mask, values, 0.0), axis=1, keepdims=True)
        return jnp.broadcast_to(column, (seqs, batch))

    above = lax.broadcasted_iota(jnp.int32, (batch, batch), 0)
    across = lax.broadcasted_iota(jnp.int32, (batch, batch), 1)
    ahead = dot(lengths.astype(BF16), (above < across).astype(BF16), (1, 0))[:1]
    slot = lax.broadcasted_iota(jnp.int32, (slots, batch), 0).astype(F32)
    for t in range(span):
        target = jnp.where(lengths[:1] > t, ahead + t, -1.0)
        picker_ref[:, t * batch : (t + 1) * batch] = (slot == target).astype(BF16)
    flat = jnp.concatenate([flat_ref[t] for t in range(span)], axis=1)
    packed = dot(flat, picker_ref[...], (1, 1)).astype(BF16)
    for k in range(sent_ref.shape[0]):
        sent_ref[k] = packed
    table_ref[0] = lengths
    table_ref[1] = chosen(own, lengths)
    table_ref[2] = chosen(mine, jnp.broadcast_to(rate_ref[...], (seqs, heads)))
    table_ref[3] = chosen(mine, jnp.broadcast_to(bias_ref[...], (seqs, heads)))
    table_ref[4] = jnp.broadcast_to(gain_out_ref[...], (seqs, batch))


def prepare(seqs, slots, *arrays):
    flat, gain = arrays[0], arrays[4]
    span, own, batch = flat.shape
    return pl.pallas_call(
        prepare_kernel,
        out_shape=(
            jax.ShapeDtypeStruct((lax.axis_size(Z), own, slots), BF16),
            jax.ShapeDtypeStruct((8, gain.shape[1]), F32),
            jax.ShapeDtypeStruct((5, seqs, batch), F32),
            jax.ShapeDtypeStruct((slots, span * batch), BF16),
        ),
        in_specs=full(len(arrays)),
        out_specs=tuple(full(4)),
        compiler_params=PARAMS,
        cost_estimate=COST,
        name="prepare",
    )(*arrays)


def project_kernel(
    x_ref, gain_ref, picker_ref, wq_ref, wk_ref, wv_ref, wb_ref, wa_ref, out_ref
):
    kv_count, local_rows, _ = out_ref.shape
    slots, rows = picker_ref.shape
    batch = 128
    span = rows // batch
    seqs = local_rows // span
    heads = wb_ref.shape[0]
    head = lax.axis_index(Z) * lax.axis_size("c") + lax.axis_index("c")
    width = gain_ref.shape[1]
    start = pl.multiple_of(lax.axis_index("kv") * width, width)
    own_head = lax.broadcasted_iota(jnp.int32, (heads, width), 0) == head

    def own_row(ref):
        tile = ref[:, pl.ds(start, width)].astype(F32)
        return jnp.sum(jnp.where(own_head, tile, 0.0), axis=0, keepdims=True)

    row = lax.broadcasted_iota(jnp.int32, (128, width), 0)
    small = jnp.where(row == 0, own_row(wb_ref), jnp.where(row == 1, own_row(wa_ref), 0.0))
    small = small.astype(BF16)
    weights = jnp.concatenate([wq_ref[...], wk_ref[...], wv_ref[...]], axis=1)
    lane = lax.broadcasted_iota(jnp.int32, (slots, 128), 1)
    normed, squares = normed_rows(features_of(x_ref), gain_ref[0:1])
    extra = jnp.where(lane == 2, squares, dot(normed, small, (1, 1))).astype(BF16)
    packed = jnp.concatenate([dot(normed, weights, (1, 0)).astype(BF16), extra], axis=1)
    placed = dot(picker_ref[...], packed, (0, 0))
    for t in range(span):
        block = placed[t * batch : (t + 1) * batch].reshape(kv_count, seqs, -1)
        out_ref[:, t * seqs : (t + 1) * seqs] = block.astype(BF16)


def project(x, gain, picker, wq, wk, wv, wb, wa, kv_count):
    rows = picker.shape[1]
    return pl.pallas_call(
        project_kernel,
        out_shape=jax.ShapeDtypeStruct((kv_count, rows // kv_count, 512), BF16),
        in_specs=full(8),
        out_specs=pl.BlockSpec(memory_space=pltpu.VMEM),
        compiler_params=PARAMS,
        name="project",
    )(x, gain, picker, wq, wk, wv, wb, wa)


def delta_kernel(recv_ref, state_ref, table_ref, head_ref, new_ref):
    seq_count, size, _ = state_ref.shape
    rows = recv_ref.shape[1]
    span = rows // seq_count
    sums = recv_ref[0].astype(F32)
    for k in range(1, recv_ref.shape[0]):
        sums = sums + recv_ref[k].astype(F32)

    def lanes(column):
        return jnp.broadcast_to(column, (rows, size))

    row_scale = lanes(lax.rsqrt(sums[:, 386:387] / D + EPSILON))
    row = lax.broadcasted_iota(jnp.int32, (rows, size), 0)
    step = row // seq_count
    seq = row % seq_count

    def every_step(k):
        return jnp.concatenate([table_ref[k]] * span, axis=0)

    live = step.astype(F32) < every_step(1)
    beta = jnp.where(live, jax.nn.sigmoid(lanes(sums[:, 384:385]) * row_scale), 0.0)
    pre = lanes(sums[:, 385:386]) * row_scale + every_step(3)
    soft = jnp.maximum(pre, 0.0) + jnp.log1p(jnp.exp(-jnp.abs(pre)))
    log_decay = jnp.where(live, -every_step(2) * soft, 0.0)

    def unit(block):
        v = sums[:, block * size : (block + 1) * size] * row_scale
        return v * lax.rsqrt(jnp.sum(v * v, axis=1, keepdims=True) + EPSILON)

    queries = unit(0) * HEAD_DIM ** (-0.5)
    keys = unit(1)
    values = sums[:, 2 * size : 3 * size] * row_scale

    def back(x, d):
        return pltpu.roll(x, d * seq_count, 0)

    cumulative, tail = log_decay, jnp.zeros_like(log_decay)
    gaps = [jnp.zeros_like(log_decay)]
    for d in range(1, span):
        gaps.append(jnp.where(step >= d, log_decay + back(gaps[-1], 1), 0.0))
        cumulative = cumulative + jnp.where(step >= d, back(log_decay, d), 0.0)
        tail = tail + jnp.where(step < span - d, back(log_decay, span - d), 0.0)
    decays = [jnp.exp(g) for g in gaps]
    grown = jnp.exp(cumulative)

    both_high, both_low = split_high_low(jnp.concatenate([keys, queries], axis=0))
    both_rows = jnp.concatenate(
        [
            jnp.concatenate([both_high, both_high], axis=1),
            jnp.concatenate([both_low, jnp.zeros_like(both_low)], axis=1),
        ],
        axis=0,
    )
    key_state = jnp.zeros_like(keys)
    query_state = jnp.zeros_like(keys)
    for n in range(0, seq_count, 2):
        halves = split_high_low(jnp.concatenate([state_ref[n], state_ref[n + 1]], axis=1))
        terms = dot(both_rows, jnp.concatenate(halves, axis=0), (1, 0))
        terms = terms[: 2 * rows] + terms[2 * rows :]
        for k in range(2):
            at = slice(k * size, (k + 1) * size)
            key_state = jnp.where(seq == n + k, terms[:rows, at], key_state)
            query_state = jnp.where(seq == n + k, terms[rows:, at], query_state)

    base = beta * (values - grown * key_state)
    lower, upper = [None], []
    for d in range(span):
        shifted = back(keys, d) if d else keys
        weight = jnp.where(step >= d, decays[d], 0.0)
        upper.append(weight * jnp.sum(queries * shifted, axis=1, keepdims=True))
        if d:
            lower.append(weight * beta * jnp.sum(keys * shifted, axis=1, keepdims=True))
    update = base
    for t in range(1, span):
        now = base
        for d in range(1, t + 1):
            now = now - lower[d] * back(update, d)
        update = jnp.where(step == t, now, update)
    attended = grown * query_state + upper[0] * update
    for d in range(1, span):
        attended = attended + upper[d] * back(update, d)
    out = attended * lax.rsqrt(jnp.mean(attended * attended, axis=1, keepdims=True) + EPSILON)
    out = (out * every_step(4)).astype(BF16)
    for k in range(head_ref.shape[0]):
        head_ref[k] = out

    k_high, k_low = split_high_low((keys * jnp.exp(tail)).T)
    k_all = jnp.concatenate([k_high, k_low, k_high], axis=1)
    for n in range(0, seq_count, 2):
        pair = [jnp.where(seq == n + k, update, 0.0) for k in range(2)]
        u_high, u_low = split_high_low(jnp.concatenate(pair, axis=1))
        added = dot(k_all, jnp.concatenate([u_high, u_high, u_low], axis=0), (1, 0))
        for k in range(2):
            last = rows - seq_count + n + k
            kept = state_ref[n + k] * grown[last : last + 1, :]
            new_ref[n + k] = kept + added[:, k * size : (k + 1) * size]


def delta_step(recv, state, table):
    kv_count, rows, _ = recv.shape
    size = state.shape[1]
    return pl.pallas_call(
        delta_kernel,
        out_shape=(
            jax.ShapeDtypeStruct((kv_count, rows, size), BF16),
            jax.ShapeDtypeStruct(state.shape, F32),
        ),
        in_specs=full(3),
        out_specs=tuple(full(2)),
        compiler_params=PARAMS,
        name="delta",
    )(recv, state, table)


def attend_kernel(heads_ref, picker_ref, w_ref, part_ref):
    kv_count, local_rows, size = heads_ref.shape
    span = picker_ref.shape[1] // 128
    seqs = local_rows // span
    heads = heads_ref[...].astype(F32)
    heads = jnp.concatenate(
        [
            heads[:, t * seqs : (t + 1) * seqs].reshape(kv_count * seqs, size)
            for t in range(span)
        ],
        axis=0,
    ).astype(BF16)
    packed = dot(picker_ref[...], heads, (1, 0)).astype(BF16)
    part_ref[...] = dot(packed, w_ref[...], (1, 0)).T.astype(BF16)


def attend(heads, picker, w_out):
    return pl.pallas_call(
        attend_kernel,
        out_shape=jax.ShapeDtypeStruct((w_out.shape[1], picker.shape[0]), BF16),
        in_specs=full(3),
        out_specs=pl.BlockSpec(memory_space=pltpu.VMEM),
        compiler_params=PARAMS,
        name="attend",
    )(heads, picker, w_out)


def gate_kernel(x_ref, gain_ref, wg_ref, wu_ref, out_ref):
    kv_count, local, wide = out_ref.shape
    units = wg_ref.shape[0]
    normed, squares = normed_rows(features_of(x_ref), gain_ref[1:2])

    def put(at, value):
        width = value.shape[1]
        out_ref[:, :, at : at + width] = value.astype(BF16).reshape(kv_count, local, width)

    half = wide // 2
    put(0, dot(normed, wg_ref[...], (1, 1)))
    put(half, dot(normed, wu_ref[...], (1, 1)))
    put(units, jnp.broadcast_to(squares, (x_ref.shape[3], half - units)))


def gate(x, gain, w_gate, w_up, kv_count):
    rows = x.shape[-1]
    return pl.pallas_call(
        gate_kernel,
        out_shape=jax.ShapeDtypeStruct((kv_count, rows // kv_count, 768), BF16),
        in_specs=full(4),
        out_specs=pl.BlockSpec(memory_space=pltpu.VMEM),
        compiler_params=PARAMS,
        name="gate",
    )(x, gain, w_gate, w_up)


def finish_kernel(recv_ref, middle_ref, picker_ref, state_ref, out_ref, new_ref, sem):
    copy = pltpu.make_async_copy(state_ref, new_ref, sem)
    copy.start()
    total = middle_ref[...].astype(F32)
    for k in range(recv_ref.shape[0]):
        total = total + recv_ref[k].astype(F32)
    span, _, batch = out_ref.shape
    spread_out = dot(total.astype(BF16), picker_ref[...], (1, 0)).astype(BF16)
    for t in range(span):
        out_ref[t] = spread_out[:, t * batch : (t + 1) * batch]
    copy.wait()


def finish(recv, middle, picker, state, span):
    own = middle.shape[0]
    return pl.pallas_call(
        finish_kernel,
        out_shape=(
            jax.ShapeDtypeStruct((span, own, picker.shape[1] // span), BF16),
            jax.ShapeDtypeStruct(state.shape, F32),
        ),
        in_specs=full(4),
        out_specs=(pl.BlockSpec(memory_space=pltpu.VMEM), pl.BlockSpec(memory_space=pl.ANY)),
        scratch_shapes=[pltpu.SemaphoreType.DMA],
        compiler_params=PARAMS,
        name="finish",
    )(recv, middle, picker, state)


def body(
    tokens,
    lengths,
    state,
    attn_gain,
    w_query,
    w_key,
    w_value,
    w_beta,
    w_alpha,
    decay_rate,
    decay_bias,
    out_gain,
    w_out,
    mix_gain,
    w_gate,
    w_up,
    w_down,
):
    kv_count = lax.axis_size("kv")
    slots = 256

    core = lax.axis_index("c").astype(jnp.uint32)
    flat, core = lax.optimization_barrier((tokens.transpose(1, 2, 0), core))
    sent, gains, table, picker = prepare(
        state.shape[0],
        slots,
        flat,
        lengths[None, :],
        decay_rate[None, :],
        decay_bias[None, :],
        attn_gain[None, :],
        mix_gain[None, :],
        out_gain[None, :],
    )
    every = lax.all_gather(swap(sent, Z), "c", axis=0, tiled=False)
    sums = project(
        every, gains, picker, w_query, w_key, w_value, w_beta.T, w_alpha.T, kv_count
    )
    heads, updated = delta_step(swap(sums, "kv"), state, table)
    attn_part = attend(swap(heads, "kv"), picker, w_out)
    attn_own = swap(pair_sum(attn_part, core), Z).astype(F32).sum(axis=0)
    middle = lax.optimization_barrier((sent[0].astype(F32) + attn_own).astype(BF16))
    middle_rows = lax.all_gather(spread(middle, Z), "c", axis=0, tiled=False)
    share = gate(middle_rows, gains, w_gate.T, w_up.T, kv_count)
    share = swap(share, "kv").astype(F32).sum(axis=0)
    units = w_gate.shape[1]
    share_scale = lax.rsqrt(share[:, units : units + 1] / D + EPSILON)
    hidden = (
        jax.nn.silu(share[:, :units] * share_scale)
        * (share[:, 384 : 384 + units] * share_scale)
    ).astype(BF16)
    hidden_every = spread(hidden, "kv").reshape(slots, units)
    down_part = dot(w_down, hidden_every, (0, 1)).astype(BF16)
    mixed, new_state = finish(
        swap(pair_sum(down_part, core), Z), middle, picker, updated, flat.shape[0]
    )
    return (mixed.transpose(2, 0, 1), new_state)


def solution(mesh):
    tp = ("z", "c")
    split = Mesh(mesh.devices.reshape(mesh.shape["kv"], -1, 2), ("kv", *tp))
    return jax.shard_map(
        body,
        mesh=split,
        in_specs=(
            P(None, None, ("kv", *tp)),
            P(),
            P("kv", None, tp),
            P("kv"),
            P("kv", tp),
            P("kv", tp),
            P("kv", tp),
            P(),
            P(),
            P(),
            P(),
            P(),
            P(tp, "kv"),
            P("kv"),
            P("kv", tp),
            P("kv", tp),
            P(tp, "kv"),
        ),
        out_specs=(P(None, None, ("kv", *tp)), P("kv", None, tp)),
        check_vma=False,
    )
```

```python
import jax
import jax.numpy as jnp
from jax import lax
from jax.experimental import pallas as pl
from jax.experimental.pallas import tpu as pltpu
from jax.sharding import Mesh, PartitionSpec as P

D = 4096
HEAD_DIM = 128
EPSILON = 1e-06
F32 = jnp.float32
BF16 = jnp.bfloat16
Z = "z"
COST = pl.CostEstimate(flops=1 << 28, bytes_accessed=1 << 21, transcendentals=0)
PARAMS = pltpu.CompilerParams(vmem_limit_bytes=12 * 1024 * 1024)


def swap(tiles, axis):
    return lax.all_to_all(tiles, axis, split_axis=0, concat_axis=0, tiled=True)


def spread(shard, axis):
    return swap(jnp.broadcast_to(shard[None], (lax.axis_size(axis), *shard.shape)), axis)


def pair_sum(part, core):
    feats, rows = part.shape
    z_count, c_count = lax.axis_size(Z), lax.axis_size("c")
    pair = lax.all_gather(part, "c", axis=0, tiled=False)
    pair = pair.reshape(c_count, z_count, c_count, -1, rows)
    mine = lax.dynamic_index_in_dim(pair, core, 2, keepdims=False)
    return mine.astype(F32).sum(axis=0).astype(BF16)


def dot(a, b, dims):
    return lax.dot_general(a, b, ((dims[:1], dims[1:]), ((), ())), preferred_element_type=F32)


def split_high_low(x):
    high = x.astype(BF16)
    return high, (x - high.astype(F32)).astype(BF16)


def full(shape_of):
    return [pl.BlockSpec(memory_space=pltpu.VMEM)] * shape_of


def features_of(ref, *at):
    c_count, z_count = ref.shape[:2]
    tiles = [ref[(c, z, *at)].astype(F32) for z in range(z_count) for c in range(c_count)]
    return jnp.concatenate(tiles, axis=0).T


def normed_rows(x, gain):
    return (x * gain).astype(BF16), jnp.sum(x * x, axis=1, keepdims=True)


def prepare_kernel(
    flat_ref,
    lengths_ref,
    rate_ref,
    bias_ref,
    gain_in_ref,
    gain_mid_ref,
    gain_out_ref,
    sent_ref,
    gains_ref,
    table_ref,
    picker_ref,
    own_picker_ref,
):
    seqs, batch = table_ref.shape[1:]
    span = flat_ref.shape[0]
    slots = picker_ref.shape[0]
    heads = rate_ref.shape[1]
    first = lax.axis_index("kv") * seqs
    head = lax.axis_index(Z) * lax.axis_size("c") + lax.axis_index("c")
    gains_ref[0:1] = gain_in_ref[...]
    gains_ref[1:2] = gain_mid_ref[...]
    lengths = jnp.broadcast_to(lengths_ref[...].astype(F32), (seqs, batch))
    own = lax.broadcasted_iota(jnp.int32, (seqs, batch), 1)
    own = own == first + lax.broadcasted_iota(jnp.int32, (seqs, batch), 0)
    mine = lax.broadcasted_iota(jnp.int32, (seqs, heads), 1) == head

    def chosen(mask, values):
        column = jnp.sum(jnp.where(mask, values, 0.0), axis=1, keepdims=True)
        return jnp.broadcast_to(column, (seqs, batch))

    above = lax.broadcasted_iota(jnp.int32, (batch, batch), 0)
    across = lax.broadcasted_iota(jnp.int32, (batch, batch), 1)
    ahead = dot(lengths.astype(BF16), (above < across).astype(BF16), (1, 0))[:1]
    slot = lax.broadcasted_iota(jnp.int32, (slots, batch), 0).astype(F32)
    for t in range(span):
        target = jnp.where(lengths[:1] > t, ahead + t, -1.0)
        picker_ref[:, t * batch : (t + 1) * batch] = (slot == target).astype(BF16)
    rows = own_picker_ref.shape[1]
    place = lax.broadcasted_iota(jnp.int32, (batch, rows), 1)
    place_seq = place // (span * seqs) * seqs + place % seqs
    other = lax.broadcasted_iota(jnp.int32, (batch, rows), 0)
    sizes = lengths.astype(BF16)
    ahead = dot(sizes, (other < place_seq).astype(BF16), (1, 0))[:1]
    limit = dot(sizes, (other == place_seq).astype(BF16), (1, 0))[:1]
    step = (place[:1] // seqs % span).astype(F32)
    target = jnp.where(limit > step, ahead + step, -1.0)
    slot = lax.broadcasted_iota(jnp.int32, (slots, rows), 0).astype(F32)
    own_picker_ref[...] = (slot == target).astype(BF16)
    flat = jnp.concatenate([flat_ref[t] for t in range(span)], axis=1)
    packed = dot(flat, picker_ref[...], (1, 1)).astype(BF16)
    for k in range(sent_ref.shape[0]):
        sent_ref[k] = packed
    table_ref[0] = lengths
    table_ref[1] = chosen(own, lengths)
    table_ref[2] = chosen(mine, jnp.broadcast_to(rate_ref[...], (seqs, heads)))
    table_ref[3] = chosen(mine, jnp.broadcast_to(bias_ref[...], (seqs, heads)))
    table_ref[4] = jnp.broadcast_to(gain_out_ref[...], (seqs, batch))


def prepare(seqs, slots, *arrays):
    flat, gain = arrays[0], arrays[4]
    span, own, batch = flat.shape
    return pl.pallas_call(
        prepare_kernel,
        out_shape=(
            jax.ShapeDtypeStruct((lax.axis_size(Z), own, slots), BF16),
            jax.ShapeDtypeStruct((8, gain.shape[1]), F32),
            jax.ShapeDtypeStruct((5, seqs, batch), F32),
            jax.ShapeDtypeStruct((slots, span * batch), BF16),
            jax.ShapeDtypeStruct((slots, span * batch), BF16),
        ),
        in_specs=full(len(arrays)),
        out_specs=tuple(full(5)),
        compiler_params=PARAMS,
        cost_estimate=COST,
        name="prepare",
    )(*arrays)


def project_kernel(
    x_ref, gain_ref, picker_ref, wq_ref, wk_ref, wv_ref, wb_ref, wa_ref, out_ref
):
    kv_count = out_ref.shape[0]
    rows = picker_ref.shape[1]
    heads = wb_ref.shape[0]
    head = lax.axis_index(Z) * lax.axis_size("c") + lax.axis_index("c")
    width = gain_ref.shape[1]
    start = pl.multiple_of(lax.axis_index("kv") * width, width)
    own_head = lax.broadcasted_iota(jnp.int32, (heads, width), 0) == head

    def own_row(ref):
        tile = ref[:, pl.ds(start, width)].astype(F32)
        return jnp.sum(jnp.where(own_head, tile, 0.0), axis=0, keepdims=True)

    row = lax.broadcasted_iota(jnp.int32, (8, width), 0)
    small = jnp.where(row == 0, own_row(wb_ref), jnp.where(row == 1, own_row(wa_ref), 0.0))
    small = small.astype(BF16)
    weights = jnp.concatenate([wq_ref[...], wk_ref[...], wv_ref[...]], axis=1)
    x = features_of(x_ref)
    normed = (x * gain_ref[0:1]).astype(BF16)
    ones = (row == 2).astype(BF16)
    extra = dot(small, normed, (1, 1)) + dot(ones, (x * x).astype(BF16), (1, 1))
    extra = dot(extra.astype(BF16), picker_ref[...], (1, 0)).astype(BF16)
    placed = dot(picker_ref[...], dot(normed, weights, (1, 0)).astype(BF16), (0, 0))
    local = rows // kv_count
    for k in range(3):
        block = placed[:, k * 128 : (k + 1) * 128].reshape(kv_count, local, 128)
        out_ref[:, k * local : (k + 1) * local] = block.astype(BF16)
    for k in range(kv_count):
        tile = k * local // 128
        out_ref[k, 3 * local :] = extra[:, tile * 128 : (tile + 1) * 128]


def project(x, gain, picker, wq, wk, wv, wb, wa, kv_count):
    rows = picker.shape[1]
    return pl.pallas_call(
        project_kernel,
        out_shape=jax.ShapeDtypeStruct((kv_count, 3 * rows // kv_count + 8, 128), BF16),
        in_specs=full(8),
        out_specs=pl.BlockSpec(memory_space=pltpu.VMEM),
        compiler_params=PARAMS,
        name="project",
    )(x, gain, picker, wq, wk, wv, wb, wa)


def delta_kernel(recv_ref, state_ref, table_ref, head_ref, new_ref, extra_ref):
    seq_count, size, _ = state_ref.shape
    rows = head_ref.shape[1]
    span = rows // seq_count
    sums = recv_ref[0].astype(F32)
    for k in range(1, recv_ref.shape[0]):
        sums = sums + recv_ref[k].astype(F32)

    def lanes(column):
        return jnp.broadcast_to(column, (rows, size))

    extra_ref[...] = sums[3 * rows :].T
    per_tile = extra_ref.shape[0] // rows
    start = pl.multiple_of(lax.axis_index("kv") % per_tile * rows, rows)
    extra = extra_ref[pl.ds(start, rows)]
    row_scale = lanes(lax.rsqrt(extra[:, 2:3] / D + EPSILON))
    row = lax.broadcasted_iota(jnp.int32, (rows, size), 0)
    step = row // seq_count
    seq = row % seq_count

    def every_step(k):
        return jnp.concatenate([table_ref[k]] * span, axis=0)

    live = step.astype(F32) < every_step(1)
    beta = jnp.where(live, jax.nn.sigmoid(lanes(extra[:, 0:1]) * row_scale), 0.0)
    pre = lanes(extra[:, 1:2]) * row_scale + every_step(3)
    soft = jnp.maximum(pre, 0.0) + jnp.log1p(jnp.exp(-jnp.abs(pre)))
    log_decay = jnp.where(live, -every_step(2) * soft, 0.0)

    def unit(block):
        v = sums[block * rows : (block + 1) * rows] * row_scale
        return v * lax.rsqrt(jnp.sum(v * v, axis=1, keepdims=True) + EPSILON)

    queries = unit(0) * HEAD_DIM ** (-0.5)
    keys = unit(1)
    values = sums[2 * rows : 3 * rows] * row_scale

    def back(x, d):
        return pltpu.roll(x, d * seq_count, 0)

    cumulative, tail = log_decay, jnp.zeros_like(log_decay)
    gaps = [jnp.zeros_like(log_decay)]
    for d in range(1, span):
        gaps.append(jnp.where(step >= d, log_decay + back(gaps[-1], 1), 0.0))
        cumulative = cumulative + jnp.where(step >= d, back(log_decay, d), 0.0)
        tail = tail + jnp.where(step < span - d, back(log_decay, span - d), 0.0)
    decays = [jnp.exp(g) for g in gaps]
    grown = jnp.exp(cumulative)

    both_high, both_low = split_high_low(jnp.concatenate([keys, queries], axis=0))
    both_rows = jnp.concatenate(
        [
            jnp.concatenate([both_high, both_high], axis=1),
            jnp.concatenate([both_low, jnp.zeros_like(both_low)], axis=1),
        ],
        axis=0,
    )
    key_state = jnp.zeros_like(keys)
    query_state = jnp.zeros_like(keys)
    for n in range(0, seq_count, 2):
        halves = split_high_low(jnp.concatenate([state_ref[n], state_ref[n + 1]], axis=1))
        terms = dot(both_rows, jnp.concatenate(halves, axis=0), (1, 0))
        terms = terms[: 2 * rows] + terms[2 * rows :]
        for k in range(2):
            at = slice(k * size, (k + 1) * size)
            key_state = jnp.where(seq == n + k, terms[:rows, at], key_state)
            query_state = jnp.where(seq == n + k, terms[rows:, at], query_state)

    base = beta * (values - grown * key_state)
    lower, upper = [None], []
    for d in range(span):
        shifted = back(keys, d) if d else keys
        weight = jnp.where(step >= d, decays[d], 0.0)
        upper.append(weight * jnp.sum(queries * shifted, axis=1, keepdims=True))
        if d:
            lower.append(weight * beta * jnp.sum(keys * shifted, axis=1, keepdims=True))
    update = base
    for t in range(1, span):
        now = base
        for d in range(1, t + 1):
            now = now - lower[d] * back(update, d)
        update = jnp.where(step == t, now, update)
    attended = grown * query_state + upper[0] * update
    for d in range(1, span):
        attended = attended + upper[d] * back(update, d)
    out = attended * lax.rsqrt(jnp.mean(attended * attended, axis=1, keepdims=True) + EPSILON)
    out = (out * every_step(4)).astype(BF16)
    for k in range(head_ref.shape[0]):
        head_ref[k] = out

    k_high, k_low = split_high_low((keys * jnp.exp(tail)).T)
    k_all = jnp.concatenate([k_high, k_low, k_high], axis=1)
    for n in range(0, seq_count, 2):
        pair = [jnp.where(seq == n + k, update, 0.0) for k in range(2)]
        u_high, u_low = split_high_low(jnp.concatenate(pair, axis=1))
        added = dot(k_all, jnp.concatenate([u_high, u_high, u_low], axis=0), (1, 0))
        for k in range(2):
            last = rows - seq_count + n + k
            kept = state_ref[n + k] * grown[last : last + 1, :]
            new_ref[n + k] = kept + added[:, k * size : (k + 1) * size]


def delta_step(recv, state, table):
    kv_count, sent_rows, size = recv.shape
    return pl.pallas_call(
        delta_kernel,
        out_shape=(
            jax.ShapeDtypeStruct((kv_count, (sent_rows - 8) // 3, size), BF16),
            jax.ShapeDtypeStruct(state.shape, F32),
        ),
        in_specs=full(3),
        out_specs=tuple(full(2)),
        scratch_shapes=[pltpu.VMEM((size, 8), F32)],
        compiler_params=PARAMS,
        name="delta",
    )(recv, state, table)


def attend_kernel(heads_ref, picker_ref, w_ref, part_ref):
    heads = heads_ref[...].reshape(picker_ref.shape[1], heads_ref.shape[2])
    packed = dot(picker_ref[...], heads, (1, 0)).astype(BF16)
    part_ref[...] = dot(packed, w_ref[...], (1, 0)).T.astype(BF16)


def attend(heads, picker, w_out):
    return pl.pallas_call(
        attend_kernel,
        out_shape=jax.ShapeDtypeStruct((w_out.shape[1], picker.shape[0]), BF16),
        in_specs=full(3),
        out_specs=pl.BlockSpec(memory_space=pltpu.VMEM),
        compiler_params=PARAMS,
        name="attend",
    )(heads, picker, w_out)


def gate_kernel(x_ref, gain_ref, wg_ref, wu_ref, out_ref):
    kv_count, local, wide = out_ref.shape
    units = wg_ref.shape[0]
    normed, squares = normed_rows(features_of(x_ref), gain_ref[1:2])

    def put(at, value):
        width = value.shape[1]
        out_ref[:, :, at : at + width] = value.astype(BF16).reshape(kv_count, local, width)

    half = wide // 2
    put(0, dot(normed, wg_ref[...], (1, 1)))
    put(half, dot(normed, wu_ref[...], (1, 1)))
    put(units, jnp.broadcast_to(squares, (x_ref.shape[3], half - units)))


def gate(x, gain, w_gate, w_up, kv_count):
    rows = x.shape[-1]
    return pl.pallas_call(
        gate_kernel,
        out_shape=jax.ShapeDtypeStruct((kv_count, rows // kv_count, 768), BF16),
        in_specs=full(4),
        out_specs=pl.BlockSpec(memory_space=pltpu.VMEM),
        compiler_params=PARAMS,
        name="gate",
    )(x, gain, w_gate, w_up)


def finish_kernel(
    recv_ref, middle_ref, picker_ref, state_ref, out_ref, new_ref, local, sem_out, sem_new
):
    state_copy = pltpu.make_async_copy(state_ref, new_ref, sem_new)
    state_copy.start()
    total = middle_ref[...].astype(F32)
    for k in range(recv_ref.shape[0]):
        total = total + recv_ref[k].astype(F32)
    span, _, batch = local.shape
    spread_out = dot(total.astype(BF16), picker_ref[...], (1, 0)).astype(BF16)
    for t in range(span):
        local[t] = spread_out[:, t * batch : (t + 1) * batch]
    out_copy = pltpu.make_async_copy(local, out_ref, sem_out)
    out_copy.start()
    out_copy.wait()
    state_copy.wait()


def finish(recv, middle, picker, state, span):
    mixed = (span, middle.shape[0], picker.shape[1] // span)
    return pl.pallas_call(
        finish_kernel,
        out_shape=(
            jax.ShapeDtypeStruct(mixed, BF16),
            jax.ShapeDtypeStruct(state.shape, F32),
        ),
        in_specs=full(4),
        out_specs=(pl.BlockSpec(memory_space=pl.ANY),) * 2,
        scratch_shapes=[
            pltpu.VMEM(mixed, BF16),
            pltpu.SemaphoreType.DMA,
            pltpu.SemaphoreType.DMA,
        ],
        compiler_params=PARAMS,
        name="finish",
    )(recv, middle, picker, state)


def body(
    tokens,
    lengths,
    state,
    attn_gain,
    w_query,
    w_key,
    w_value,
    w_beta,
    w_alpha,
    decay_rate,
    decay_bias,
    out_gain,
    w_out,
    mix_gain,
    w_gate,
    w_up,
    w_down,
):
    kv_count = lax.axis_size("kv")
    slots = 256

    core = lax.axis_index("c").astype(jnp.uint32)
    flat, core = lax.optimization_barrier((tokens.transpose(1, 2, 0), core))
    sent, gains, table, picker, own_picker = prepare(
        state.shape[0],
        slots,
        flat,
        lengths[None, :],
        decay_rate[None, :],
        decay_bias[None, :],
        attn_gain[None, :],
        mix_gain[None, :],
        out_gain[None, :],
    )
    every = lax.all_gather(swap(sent, Z), "c", axis=0, tiled=False)
    sums = project(
        every, gains, own_picker, w_query, w_key, w_value, w_beta.T, w_alpha.T, kv_count
    )
    heads, updated = delta_step(swap(sums, "kv"), state, table)
    attn_part = attend(swap(heads, "kv"), own_picker, w_out)
    attn_own = swap(pair_sum(attn_part, core), Z).astype(F32).sum(axis=0)
    middle = lax.optimization_barrier((sent[0].astype(F32) + attn_own).astype(BF16))
    middle_rows = lax.all_gather(spread(middle, Z), "c", axis=0, tiled=False)
    share = gate(middle_rows, gains, w_gate.T, w_up.T, kv_count)
    share = swap(share, "kv").astype(F32).sum(axis=0)
    units = w_gate.shape[1]
    share_scale = lax.rsqrt(share[:, units : units + 1] / D + EPSILON)
    hidden = (
        jax.nn.silu(share[:, :units] * share_scale)
        * (share[:, 384 : 384 + units] * share_scale)
    ).astype(BF16)
    hidden_every = spread(hidden, "kv").reshape(slots, units)
    down_part = dot(w_down, hidden_every, (0, 1)).astype(BF16)
    mixed, new_state = finish(
        swap(pair_sum(down_part, core), Z), middle, picker, updated, flat.shape[0]
    )
    return (mixed.transpose(2, 0, 1), new_state)


def solution(mesh):
    tp = ("z", "c")
    split = Mesh(mesh.devices.reshape(mesh.shape["kv"], -1, 2), ("kv", *tp))
    return jax.shard_map(
        body,
        mesh=split,
        in_specs=(
            P(None, None, ("kv", *tp)),
            P(),
            P("kv", None, tp),
            P("kv"),
            P("kv", tp),
            P("kv", tp),
            P("kv", tp),
            P(),
            P(),
            P(),
            P(),
            P(),
            P(tp, "kv"),
            P("kv"),
            P("kv", tp),
            P("kv", tp),
            P(tp, "kv"),
        ),
        out_specs=(P(None, None, ("kv", *tp)), P("kv", None, tp)),
        check_vma=False,
    )
```
